256 devices in a mesh: ep: 16 (over y, x), tp: 16 (over z, core).
Axes of the slice: x: 4, y: 4, z: 8, core: 2. Of those that a mesh axis runs over, the one named last changes fastest.
Arguments:
- pool_in: bfloat16 [131072, 1024], P(('ep', 'tp')), may hold values from -6 to 6
- pool_weight: bfloat16 [4, 256, 256], replicated, may hold values from -0.375 to 0.375
- pool_gain: float32 [1024], replicated, may hold values from 0.1 to 1.9
- out_weight: bfloat16 [1024, 2048], P('tp'), may hold values from -0.1875 to 0.1875
- mix_gain: float32 [2048], replicated, may hold values from 0.1 to 1.9
- expert_in: bfloat16 [4096, 2048], P('ep'), may hold values from -6 to 6
- routes: int32 [4096, 4], P('ep'), may hold values from 0 to 31, all different within a row; in each aligned block of 16 rows (0 to 15, 16 to 31, ...) at most 4 rows name the same one
- route_weight: float32 [4096, 4], P('ep'), may hold values from 0.1 to 1
- pre_gain: float32 [2048], replicated, may hold values from 0.1 to 1.9
- gate_weight: bfloat16 [32, 2048, 4096], P('ep', None, 'tp'), may hold values from -0.39648438 to 0.39648438
- up_weight: bfloat16 [32, 2048, 4096], P('ep', None, 'tp'), may hold values from -0.39648438 to 0.39648438
- down_weight: bfloat16 [32, 4096, 2048], P('ep', 'tp'), may hold values from -0.09375 to 0.09375
- post_gain: float32 [2048], replicated, may hold values from 0.1 to 1.9
Outputs:
- mix_out: bfloat16 [131072, 2048], P(('ep', 'tp'))
- expert_out: bfloat16 [4096, 2048], P(('ep', 'tp'))
The draws below stay inside these ranges and needn't reach their ends.
Inputs may be any that keep to these rules, and one draw needn't show every extreme that they name: `routes`: each row names 4 different experts. In each aligned block of 16 rows no expert is named by more than 4 rows, a bound that some block reaches.
All inputs are finite; a program needn't handle non-finite values.
Results may differ from the reference program's by a relative error of at most 0.019.
Values may be sent and summed in bfloat16 or wider, within the bound.
A program may use at most 128 MiB of HBM per device.

```python
import math
import jax
import jax.numpy as jnp
import numpy as np
from jax import lax

D = 2048
DP = 1024
GROUP = 256
FF = 4096
EXPERTS = 32
TOPK = 4
MOE_TOK = 4096
MIX_TOK = 131072
SUB = 16
CAP = 4
N_TP = 16


def shard_levels(rng, dims, cuts, least, high):
    level, own = 1.0, jax.random.fold_in(rng, 6)
    for dim, shards_of in cuts:
        heights = jnp.exp(jax.random.uniform(jax.random.fold_in(own, dim), (shards_of,), jnp.float32, least / len(cuts), high / len(cuts)))
        level = level * jnp.repeat(heights, dims[dim] // shards_of).reshape([-1 if axis == dim else 1 for axis in range(len(dims))])
    return level


def deal_out(rng, own, number, rows, count, top, most, lean):
    order = jax.random.permutation(rng, count)
    heavy_load, common = portions_of(count, rows * top, most, lean, True), portions_of(count, rows * top, most, lean, False)
    places = jnp.arange(count)

    def named(sizes, turn):
        used = int((sizes > 0).sum())
        fixed = max(1, used // 4)
        passed = fixed + (places - fixed + turn * (used - fixed)) % max(1, count - fixed)
        return jnp.zeros((count,), jnp.int32).at[order[jnp.where(places < fixed, places, passed)]].set(jnp.asarray(sizes, jnp.int32))

    sizes = jnp.where(number % 4 == 0, named(heavy_load, number // 4), named(common, number - number // 4 - 1))
    mixed = jax.random.permutation(jax.random.fold_in(own, 3), count)
    giver, sink = mixed[0:count // 2 * 2:2], mixed[1:count // 2 * 2:2]
    margin = jnp.minimum(sizes[giver] - 1, most - sizes[sink]) // 2
    margin = jnp.where((giver == order[0]) | (sink == order[0]) | (sizes[sink] == 0), 0, jnp.maximum(margin, 0))
    passed = jax.random.randint(jax.random.fold_in(own, 4), (count // 2,), 0, 1 << 20) % (margin + 1)
    sizes = sizes.at[giver].add(-passed).at[sink].add(passed)
    labels = jnp.searchsorted(jnp.cumsum(sizes), jnp.arange(rows * top), side="right").astype(jnp.int32)
    listing = labels.reshape(top, rows).T
    listing = listing[jax.random.permutation(jax.random.fold_in(own, 1), rows)]
    turn = jax.random.randint(jax.random.fold_in(own, 2), (rows, 1), 0, top)
    return jnp.take_along_axis(listing, (jnp.arange(top)[None, :] + turn) % top, axis=1)


def portions_of(count, total, limit, lean, full):
    portions = [(1 << 20) // math.isqrt(standing ** lean) + 1 for standing in range(1, count + 1)]
    largest = limit if full else min(limit, max(-(-total // count), total * portions[0] // sum(portions)))
    least = 1 if total - largest >= count - 1 else 0
    given, surplus = [largest] + [least] * (count - 1), total - largest - least * (count - 1)
    while surplus > 0:
        candidates = [i for i in range(1, count) if given[i] < largest] or [i for i in range(1, count) if given[i] < limit]
        pool, left = sum([portions[i] for i in candidates]), surplus
        for i in candidates:
            more = min(limit - given[i], max(1, left * portions[i] // pool), surplus)
            given[i] = given[i] + more
            surplus = surplus - more
    return np.array(given)


def noise(rng, extent, width, most, cuts=(), held_as=jnp.bfloat16):
    level = shard_levels(rng, extent, cuts, -0.22, 0.18) if cuts else 1.0
    array = jax.random.normal(rng, extent, jnp.float32) * width * level
    return jnp.minimum(jnp.maximum(array, -most), most).astype(held_as)


def setup_inputs(seed: int = 0) -> dict:
    splits = jax.random.split(jax.random.key(seed), 14)
    pool_in = noise(splits[0], (MIX_TOK, DP), 1.0, 6.0, ((0, 256),))
    pool_weight = noise(splits[1], (4, GROUP, GROUP), GROUP ** -0.5, 0.375)
    pool_gain = jnp.clip(1.0 + 0.18 * jax.random.normal(splits[2], (DP,), jnp.float32), 0.1, 1.9)
    out_weight = noise(splits[3], (DP, D), DP ** -0.5, 0.1875, ((0, 16),))
    mix_gain = jnp.clip(1.0 + 0.18 * jax.random.normal(splits[4], (D,), jnp.float32), 0.1, 1.9)
    expert_in = noise(splits[5], (MOE_TOK, D), 1.0, 6.0, ((0, 16),))
    routes_keys = jax.random.split(jax.random.fold_in(splits[6], 1), MOE_TOK // SUB)
    routes_turns = jax.random.permutation(jax.random.fold_in(splits[6], 3), MOE_TOK // SUB)
    routes = jax.vmap(lambda own, number: deal_out(jax.random.fold_in(splits[6], 2), own, number, SUB, EXPERTS, TOPK, CAP, 2))(routes_keys, routes_turns).reshape((MOE_TOK, TOPK))
    route_weight = jnp.clip(jnp.exp(math.log(1.0) - 2.3025851 * jax.random.uniform(splits[7], (MOE_TOK, TOPK), jnp.float32) ** shard_levels(splits[7], (MOE_TOK, TOPK), ((0, 16),), -0.2, 0.2)), 0.1, 1.0)
    pre_gain = jnp.clip(1.0 + 0.18 * jax.random.normal(splits[8], (D,), jnp.float32), 0.1, 1.9)
    gate_weight = noise(splits[9], (EXPERTS, D, FF), (3.0 * D ** -0.5), 0.39648438, ((0, 16), (2, 16)))
    up_weight = noise(splits[10], (EXPERTS, D, FF), (3.0 * D ** -0.5), 0.39648438, ((0, 16), (2, 16)))
    down_weight = noise(splits[11], (EXPERTS, FF, D), FF ** -0.5, 0.09375, ((0, 16), (1, 16)))
    post_gain = jnp.clip(1.0 + 0.18 * jax.random.normal(splits[12], (D,), jnp.float32), 0.1, 1.9)
    return {"pool_in": pool_in, "pool_weight": pool_weight, "pool_gain": pool_gain, "out_weight": out_weight, "mix_gain": mix_gain, "expert_in": expert_in, "routes": routes, "route_weight": route_weight, "pre_gain": pre_gain, "gate_weight": gate_weight, "up_weight": up_weight, "down_weight": down_weight, "post_gain": post_gain}


WINDOWS = (2, 4, 8, 16)
EPS = 1e-06
LIMIT = 7.0
ALPHA = 1.702

def rms_scale(values, gain):
    mean_square = lax.optimization_barrier(jnp.mean(values * values, axis=-1, keepdims=True))
    return values * lax.rsqrt(mean_square + EPS) * gain.astype(jnp.float32)

def trailing_pool(padded, first_pos, rows):
    group = padded.shape[1] // 4
    position = first_pos + jnp.arange(rows, dtype=jnp.int32)
    pieces = []
    for which, window in enumerate(WINDOWS):
        channels = padded[:, which * group:(which + 1) * group]
        running = channels[16:16 + rows]
        for reach in range(2, window + 1):
            running = running + channels[17 - reach:17 - reach + rows]
        count = jnp.minimum(position + 1, window).astype(jnp.float32)[:, None]
        pieces.append(running / count)
    pooled = jnp.concatenate(pieces, axis=1)
    return (pooled - padded[16:]).astype(jnp.bfloat16)

def selection(block_routes, experts, capacity):
    flat = block_routes.reshape(-1)
    onehot = (flat[:, None] == jnp.arange(experts, dtype=jnp.int32)[None, :]).astype(jnp.int32)
    earlier = jnp.cumsum(onehot, axis=0) - onehot
    rank = lax.optimization_barrier(jnp.sum(earlier * onehot, axis=1))
    slots = (flat * capacity + rank).reshape(block_routes.shape)
    return (slots[:, :, None] == jnp.arange(experts * capacity, dtype=jnp.int32)[None, None, :]).astype(jnp.bfloat16)

def clamped_unit(gate, up):
    gate = jnp.minimum(gate, LIMIT)
    up = jnp.clip(up, -LIMIT, LIMIT)
    return (up + 1.0) * gate * jax.nn.sigmoid(ALPHA * gate)

def expert_rows(rows, gate_w, up_w, down_w):
    gate = jnp.dot(rows, gate_w, preferred_element_type=jnp.float32)
    up = jnp.dot(rows, up_w, preferred_element_type=jnp.float32)
    hidden = clamped_unit(gate, up).astype(jnp.bfloat16)
    parts = hidden.reshape(rows.shape[0], N_TP, FF // N_TP).astype(jnp.float32)
    slices = down_w.reshape(N_TP, FF // N_TP, D).astype(jnp.float32)
    partial_value = jnp.einsum('rtf,tfd->rtd', parts, slices).astype(jnp.bfloat16)
    partial_value = lax.optimization_barrier(partial_value)
    return lax.optimization_barrier(jnp.sum(partial_value.astype(jnp.float32), axis=1)).astype(jnp.bfloat16)

def reference(pool_in, pool_weight, pool_gain, out_weight, mix_gain, expert_in, routes, route_weight, pre_gain, gate_weight, up_weight, down_weight, post_gain):
    rows = pool_in.shape[0]
    padded = jnp.concatenate([jnp.zeros((16, pool_in.shape[1]), jnp.float32), pool_in.astype(jnp.float32)], axis=0)
    diff = trailing_pool(padded, jnp.int32(0), rows)
    grouped = diff.reshape(rows, 4, GROUP).astype(jnp.float32)
    mixed = jnp.einsum('sgc,gcd->sgd', grouped, pool_weight.astype(jnp.float32))
    mixed = (mixed.reshape(rows, DP) * pool_gain.astype(jnp.float32)).astype(jnp.bfloat16)
    projected = jnp.dot(mixed, out_weight, preferred_element_type=jnp.float32)
    mix_out = rms_scale(projected, mix_gain).astype(jnp.bfloat16)
    normed = rms_scale(expert_in.astype(jnp.float32), pre_gain).astype(jnp.bfloat16)
    blocks = routes.shape[0] // SUB
    picks = jax.vmap(lambda block: selection(block, EXPERTS, CAP))(routes.reshape(blocks, SUB, TOPK)).astype(jnp.float32)
    token_picks = lax.optimization_barrier(jnp.sum(picks, axis=2))
    buffers = jnp.einsum('bts,btd->bsd', token_picks, normed.reshape(blocks, SUB, D).astype(jnp.float32)).astype(jnp.bfloat16)
    gathered = buffers.reshape(blocks, EXPERTS, CAP, D).transpose(1, 0, 2, 3).reshape(EXPERTS, blocks * CAP, D)
    outputs = lax.map(lambda operands: expert_rows(*operands), (gathered, gate_weight, up_weight, down_weight))
    back = outputs.reshape(EXPERTS, blocks, CAP, D).transpose(1, 0, 2, 3).reshape(blocks, EXPERTS * CAP, D).astype(jnp.float32)
    per_route = jnp.einsum('btks,bsd->btkd', picks, back)
    weights = route_weight.reshape(blocks, SUB, TOPK).astype(jnp.float32)
    combined = lax.optimization_barrier(jnp.sum(per_route * weights[..., None], axis=2)).reshape(blocks * SUB, D)
    expert_out = rms_scale(combined, post_gain).astype(jnp.bfloat16)
    return (mix_out, expert_out)
```

```python
import functools

import jax
import jax.numpy as jnp
from jax import lax
from jax.experimental import pallas as pl
from jax.experimental.pallas import tpu as pltpu
from jax.sharding import PartitionSpec as P

MESH = pl.DeviceIdType.MESH
WINDOWS = (2, 4, 8, 16)
EPS = 1e-06
LIMIT = 7.0
ALPHA = 1.702
F32 = jnp.float32
BF16 = jnp.bfloat16


def ring(a):
    return min(a, 4 - a)


ORDER = sorted(((a, b) for a in range(4) for b in range(4)), key=lambda t: ring(t[0]) + ring(t[1]))


def clamped_unit(gate, up):
    gate = jnp.minimum(gate, LIMIT)
    up = jnp.clip(up, -LIMIT, LIMIT)
    return (up + 1.0) * gate * jax.nn.sigmoid(ALPHA * gate)


def remote(src, dst, send, recv, device):
    return pltpu.make_async_remote_copy(
        src_ref=src, dst_ref=dst, send_sem=send, recv_sem=recv, device_id=device, device_id_type=MESH
    )


def kernel(
    pool_in, pool_weight, pool_gain, out_weight, mix_gain, expert_in, routes, route_weight, pre_gain,
    gate_weight, up_weight, down_weight, post_gain,
    mix_out, expert_out,
    xin, sendbuf, rows_in, rows_z, part_in, part_z, sums, neigh, back, mine, theirs,
    gate_w, up_w, down_w, padded, mixed, w_all, acc, staged,
    local_sem, send_a, recv_a, send_z, recv_z, send_p, recv_p, send_r, recv_r, send_t, recv_t,
    send_w, recv_w, send_o, recv_o, send_h, recv_h, out_sem,
):
    i = lax.axis_index("ep")
    j = lax.axis_index("tp")
    z, c = j // 2, j % 2
    y, x = i // 4, i % 4
    p = z % 2
    here = (i, j)
    mate = (i, 2 * z + 1 - c)

    def plane(dy, dx):
        return ((y + dy) % 4) * 4 + (x + dx) % 4

    def along(dz):
        return (i, 2 * ((z + dz) % 8) + c)

    after = (jnp.where(j == 15, (i + 1) % 16, i), (j + 1) % 16)
    before = (jnp.where(j == 0, (i + 15) % 16, i), (j + 15) % 16)

    def block_row(parity, b):
        return pl.multiple_of((2 * (parity + 2 * b) + c) * 16, 16)

    loads = []

    def load(src, dst):
        copy = pltpu.make_async_copy(src, dst, local_sem.at[len(loads)])
        copy.start()
        loads.append(copy)
        return copy

    token_loads = [
        load(expert_in.at[pl.ds(block_row(1 - p, b), 16)], xin.at[pl.ds(16 * b, 16)]) for b in range(4)
    ]
    weight_loads = [
        load(gate_weight.at[c], gate_w.at[0]),
        load(up_weight.at[c], up_w.at[0]),
        load(down_weight.at[c], down_w.at[0]),
    ]
    pool_load = load(pool_in, padded.at[pl.ds(16, 512)])
    slow, fast = jnp.where(c == 0, y, x), jnp.where(c == 0, x, y)
    w_mine = slow * 4 + fast
    w_src = out_weight.at[:, pl.ds(pl.multiple_of(i * 128, 128), 128)]
    w_load = load(w_src, w_all.at[c, w_mine, z])

    bar = pltpu.get_barrier_semaphore()

    def greet(device):
        pl.semaphore_signal(bar, inc=1, device_id=device, device_id_type=MESH)

    for dy, dx in ORDER[1:]:
        for core in range(2):
            greet((plane(dy, dx), 2 * z + core))
    for dz in range(1, 8):
        greet(along(dz))
    greet(mate)
    greet((jnp.where(c == 1, after[0], before[0]), jnp.where(c == 1, after[1], before[1])))

    lane = lax.broadcasted_iota(jnp.int32, (1, 512), 1)
    expert = jnp.zeros((1, 512), jnp.int32)
    for k, (dy, dx) in enumerate(ORDER):
        expert = jnp.where(lane // 32 == k, 2 * plane(dy, dx), expert)
    expert = expert + (lane // 16) % 2
    slot_lane = lane % 16
    token = lax.broadcasted_iota(jnp.int32, (64, 64), 0)
    other = lax.broadcasted_iota(jnp.int32, (64, 64), 1)
    earlier = jnp.where((other < token) & (other // 16 == token // 16), 1.0, 0.0).astype(BF16)
    base = (lax.broadcasted_iota(jnp.int32, (64, 1), 0) // 16) * 4

    def selection(parity, weighted):
        chosen = jnp.concatenate([routes[pl.ds(block_row(parity, b), 16), :] for b in range(4)], axis=0)
        weights = jnp.concatenate([route_weight[pl.ds(block_row(parity, b), 16), :] for b in range(4)], axis=0)
        hot = jnp.zeros((64, 512), F32)
        value = jnp.zeros((64, 512), F32)
        for k in range(4):
            match = chosen[:, k : k + 1] == expert
            hot = jnp.where(match, 1.0, hot)
            value = jnp.where(match, weights[:, k : k + 1], value)
        rank = jnp.dot(earlier, hot.astype(BF16), preferred_element_type=F32).astype(jnp.int32)
        taken = (rank + base) == slot_lane
        return jnp.where(taken, value if weighted else hot, 0.0)

    pick = selection(1 - p, False).T.astype(BF16)
    for copy in token_loads:
        copy.wait()
    tokens = xin[...].astype(F32)
    scale = lax.rsqrt(jnp.mean(tokens * tokens, axis=-1, keepdims=True) + EPS)
    normed = (tokens * scale * pre_gain[...]).astype(BF16)
    for k in range(4):
        piece = jnp.dot(pick[128 * k : 128 * k + 128], normed, preferred_element_type=F32)
        sendbuf[4 * k : 4 * k + 4] = piece.astype(BF16).reshape(4, 2, 16, 2048)

    pl.semaphore_wait(bar, 39)

    def to_plane(k, core):
        dy, dx = ORDER[k]
        return remote(
            sendbuf.at[k, core], rows_in.at[k, c], send_a.at[k, core], recv_a.at[k, c],
            (plane(dy, dx), 2 * z + core),
        )

    w_z = []
    for dz in range(1, 8):
        copy = remote(w_src, w_all.at[c, w_mine, z], send_w.at[dz], recv_w.at[dz], along(dz))
        copy.start()
        w_z.append(copy)
    for k in range(1, 16):
        for core in range(2):
            to_plane(k, core).start()
    to_mate = remote(sendbuf.at[0, 1 - c], rows_in.at[0, c], send_a.at[0, 0], recv_a.at[0, 0], mate)
    to_mate.start()
    rim = remote(pool_in.at[pl.ds(496, 16)], padded.at[pl.ds(0, 16)], send_h, recv_h, after)
    rim.start()
    swaps = [
        remote(gate_weight.at[1 - c], gate_w.at[1], send_o.at[0], recv_o.at[0], mate),
        remote(up_weight.at[1 - c], up_w.at[1], send_o.at[1], recv_o.at[1], mate),
        remote(down_weight.at[1 - c], down_w.at[1], send_o.at[2], recv_o.at[2], mate),
    ]
    for copy in swaps:
        copy.start()
    rows_in[0, c] = sendbuf[0, c]

    pool_load.wait()
    rim.wait_recv()
    number = i * 16 + j
    row = lax.broadcasted_iota(jnp.int32, (528, 1), 0)
    live = (row >= 16) | (number > 0)
    position = number * 512 + lax.broadcasted_iota(jnp.int32, (512, 1), 0)
    for g, window in enumerate(WINDOWS):
        inverse = 1.0 / jnp.minimum(position + 1, window).astype(F32)
        diffs = []
        for half in range(2):
            cols = slice(g * 256 + half * 128, g * 256 + half * 128 + 128)
            values = jnp.where(live, padded[:, cols].astype(F32), 0.0)
            total = values
            reach = 1
            while reach < window:
                total = total + pltpu.roll(total, reach, 0)
                reach *= 2
            diffs.append((total[16:] * inverse - values[16:]).astype(BF16))
        diff = jnp.concatenate(diffs, axis=1)
        out = jnp.dot(diff, pool_weight[g], preferred_element_type=F32)
        mixed[:, g * 256 : (g + 1) * 256] = (out * pool_gain[:, g * 256 : (g + 1) * 256]).astype(BF16)

    def onward(k, core):
        return remote(
            rows_in.at[k, core], rows_z.at[k, core], send_z.at[k, core], recv_z.at[k, core],
            along(1 if core == 0 else 7),
        )

    def arrive(ks):
        for k in ks:
            if k == 0:
                to_mate.wait_recv()
            for core in range(2):
                if k:
                    remote(sendbuf.at[k, core], rows_in.at[k, core], send_a.at[k, core], recv_a.at[k, core], here).wait_recv()
                onward(k, core).start()

    def experts(source, first):
        block = source[first : first + 8].reshape(256, 2048)
        hidden = []
        for half in range(2):
            gate = jnp.dot(block, gate_w[half], preferred_element_type=F32)
            up = jnp.dot(block, up_w[half], preferred_element_type=F32)
            hidden.append(clamped_unit(gate, up).astype(BF16))
        hidden = jnp.concatenate(hidden, axis=1)
        return jnp.dot(hidden, down_w[...].reshape(512, 2048), preferred_element_type=F32)

    def partial(k, core):
        return remote(
            part_in.at[k, core], neigh.at[k, core], send_p.at[k, core], recv_p.at[k, core],
            along(1 if core == 0 else 7),
        )

    def inner(first):
        part_in[first : first + 8] = experts(rows_in, first).astype(BF16).reshape(8, 2, 16, 2048)
        for k in range(first, first + 8):
            for core in range(2):
                partial(k, core).start()

    def outer(first):
        for k in range(first, first + 8):
            for core in range(2):
                onward(k, core).wait_recv()
        part_z[first : first + 8] = experts(rows_z, first).reshape(8, 2, 16, 2048)

    def w_first():
        w_load.wait()
        for copy in w_z:
            copy.wait_recv()
        for k in range(1, 4):
            w_fast(k).start()

    def w_fast(k):
        dy, dx = jnp.where(c == 0, 0, k), jnp.where(c == 0, k, 0)
        return remote(w_all.at[c, w_mine], w_all.at[c, w_mine], send_w.at[7 + k], recv_w.at[7 + k], (plane(dy, dx), j))

    def w_slow(k):
        dy, dx = jnp.where(c == 0, k, 0), jnp.where(c == 0, 0, k)
        strip = w_all.at[c, pl.ds(slow * 4, 4)]
        return remote(strip, strip, send_w.at[10 + k], recv_w.at[10 + k], (plane(dy, dx), j))

    def w_core():
        return remote(w_all.at[c], w_all.at[c], send_w.at[0], recv_w.at[0], mate)

    arrive(range(0, 4))
    w_first()
    arrive(range(4, 8))
    for copy in weight_loads:
        copy.wait()
    for copy in swaps:
        copy.wait_recv()
    inner(0)
    arrive(range(8, 12))
    outer(0)
    for k in range(1, 4):
        w_fast(k).wait_recv()
    for k in range(1, 4):
        w_slow(k).start()
    arrive(range(12, 16))
    inner(8)
    outer(8)

    def home(k, core):
        dy, dx = ORDER[k]
        return remote(
            sums.at[k, core], back.at[k, c], send_r.at[k, core], recv_r.at[k, c],
            (plane(-dy, -dx), 2 * z + core),
        )

    home_mate = remote(sums.at[0, 1 - c], back.at[0, c], send_r.at[0, 0], recv_r.at[0, 0], mate)

    def settle(ks):
        for k in ks:
            for core in range(2):
                partial(k, core).wait_recv()
            sums[k] = (part_z[k] + neigh[k].astype(F32)).astype(BF16)
            if k == 0:
                home_mate.start()
                back[0, c] = sums[0, c]
            else:
                for core in range(2):
                    home(k, core).start()

    settle(range(0, 8))
    for k in range(1, 4):
        w_slow(k).wait_recv()
    w_core().start()
    settle(range(8, 16))

    w_core().wait_recv()
    outs = []
    for h in range(2):
        rows = mixed[256 * h : 256 * h + 256]
        square = jnp.zeros((256, 1), F32)
        for n in range(8):
            sides = []
            for b in (2 * n, 2 * n + 1):
                turned = (b % 4) * 4 + b // 4
                sides.append(
                    jnp.concatenate([w_all[core, (b, turned)[core], q] for q in range(8) for core in range(2)], axis=0)
                )
            out = jnp.dot(rows, jnp.concatenate(sides, axis=1), preferred_element_type=F32)
            square = square + jnp.sum(out * out, axis=-1, keepdims=True)
            acc[:, 256 * n : 256 * n + 256] = out
        scale = lax.rsqrt(square * (1.0 / 2048.0) + EPS)
        staged[h] = (acc[...] * scale * mix_gain[...]).astype(BF16)
        copy = pltpu.make_async_copy(staged.at[h], mix_out.at[pl.ds(256 * h, 256)], out_sem.at[h])
        copy.start()
        outs.append(copy)

    weight = selection(p, True)
    high = weight.astype(BF16)
    low = (weight - high.astype(F32)).astype(BF16)
    both = jnp.concatenate([high, low], axis=0)
    home_mate.wait_recv()
    for k in range(1, 16):
        for core in range(2):
            remote(sums.at[k, core], back.at[k, core], send_r.at[k, core], recv_r.at[k, core], here).wait_recv()
    total = jnp.dot(both, back[...].reshape(512, 2048), preferred_element_type=F32)
    total = total[:64] + total[64:]
    mine[...] = total.astype(BF16).reshape(4, 16, 2048)

    def spread(m):
        return remote(
            mine.at[((z + 8 - 2 * m) % 8) // 2], theirs.at[m], send_t.at[m], recv_t.at[m], along(8 - 2 * m)
        )

    for m in (2, 1, 3):
        spread(m).start()
    acc[0:64] = total
    result = acc[pl.ds(pl.multiple_of((z // 2) * 16, 16), 16), :]
    for m in (1, 3, 2):
        spread(m).wait_recv()
        result = result + theirs[m].astype(F32)
    scale = lax.rsqrt(jnp.mean(result * result, axis=-1, keepdims=True) + EPS)
    expert_out[...] = (result * scale * post_gain[...]).astype(BF16)

    for copy in outs:
        copy.wait()
    for copy in w_z + swaps + [rim, to_mate, home_mate, w_core()]:
        copy.wait_send()
    for k in range(1, 4):
        w_fast(k).wait_send()
        w_slow(k).wait_send()
        spread(k).wait_send()
    for k in range(16):
        for core in range(2):
            onward(k, core).wait_send()
            partial(k, core).wait_send()
            if k:
                to_plane(k, core).wait_send()
                home(k, core).wait_send()


def body(
    pool_in, pool_weight, pool_gain, out_weight, mix_gain, expert_in, routes, route_weight, pre_gain,
    gate_weight, up_weight, down_weight, post_gain,
):
    vmem = pl.BlockSpec(memory_space=pltpu.VMEM)
    hbm = pl.BlockSpec(memory_space=pl.ANY)
    dma = pltpu.SemaphoreType.DMA
    tile = (16, 2, 16, 2048)
    return pl.pallas_call(
        kernel,
        out_shape=(
            jax.ShapeDtypeStruct((512, 2048), BF16),
            jax.ShapeDtypeStruct((16, 2048), BF16),
        ),
        in_specs=[hbm, vmem, vmem, hbm, vmem, hbm, vmem, vmem, vmem, hbm, hbm, hbm, vmem],
        out_specs=(hbm, vmem),
        scratch_shapes=[
            pltpu.VMEM((64, 2048), BF16),
            pltpu.VMEM(tile, BF16),
            pltpu.VMEM(tile, BF16),
            pltpu.VMEM(tile, BF16),
            pltpu.VMEM(tile, BF16),
            pltpu.VMEM(tile, F32),
            pltpu.VMEM(tile, BF16),
            pltpu.VMEM(tile, BF16),
            pltpu.VMEM(tile, BF16),
            pltpu.VMEM((4, 16, 2048), BF16),
            pltpu.VMEM((4, 16, 2048), BF16),
            pltpu.VMEM((2, 2048, 256), BF16),
            pltpu.VMEM((2, 2048, 256), BF16),
            pltpu.VMEM((2, 256, 2048), BF16),
            pltpu.VMEM((528, 1024), BF16),
            pltpu.VMEM((512, 1024), BF16),
            pltpu.VMEM((2, 16, 8, 64, 128), BF16),
            pltpu.VMEM((256, 2048), F32),
            pltpu.VMEM((2, 256, 2048), BF16),
            dma((9,)),
            dma((16, 2)), dma((16, 2)),
            dma((16, 2)), dma((16, 2)),
            dma((16, 2)), dma((16, 2)),
            dma((16, 2)), dma((16, 2)),
            dma((4,)), dma((4,)),
            dma((14,)), dma((14,)),
            dma((3,)), dma((3,)),
            dma, dma,
            dma((2,)),
        ],
        compiler_params=pltpu.CompilerParams(
            collective_id=0, has_side_effects=True, vmem_limit_bytes=60 * 1024 * 1024
        ),
        name="mixer_experts",
    )(
        pool_in, pool_weight, pool_gain.reshape(1, -1), out_weight, mix_gain.reshape(1, -1), expert_in, routes,
        route_weight, pre_gain.reshape(1, -1), gate_weight, up_weight, down_weight, post_gain.reshape(1, -1),
    )


def solution(mesh):
    return jax.shard_map(
        body,
        mesh=mesh,
        in_specs=(
            P(("ep", "tp"), None),
            P(),
            P(),
            P("tp", None),
            P(),
            P("ep", None),
            P("ep", None),
            P("ep", None),
            P(),
            P("ep", None, "tp"),
            P("ep", None, "tp"),
            P("ep", "tp", None),
            P(),
        ),
        out_specs=(P(("ep", "tp"), None), P(("ep", "tp"), None)),
        check_vma=False,
    )
```

```python
import functools

import jax
import jax.numpy as jnp
from jax import lax
from jax.experimental import pallas as pl
from jax.experimental.pallas import tpu as pltpu
from jax.sharding import PartitionSpec as P

MESH = pl.DeviceIdType.MESH
WINDOWS = (2, 4, 8, 16)
EPS = 1e-06
LIMIT = 7.0
ALPHA = 1.702
F32 = jnp.float32
BF16 = jnp.bfloat16


phase = jax.named_scope


def ring(a):
    return min(a, 4 - a)


ORDER = sorted(((a, b) for a in range(4) for b in range(4)), key=lambda t: ring(t[0]) + ring(t[1]))


def clamped_unit(gate, up):
    gate = jnp.minimum(gate, LIMIT)
    up = jnp.clip(up, -LIMIT, LIMIT)
    return (up + 1.0) * gate * jax.nn.sigmoid(ALPHA * gate)


def remote(src, dst, send, recv, device):
    return pltpu.make_async_remote_copy(
        src_ref=src, dst_ref=dst, send_sem=send, recv_sem=recv, device_id=device, device_id_type=MESH
    )


def kernel(
    pool_in, pool_weight, pool_gain, out_weight, mix_gain, expert_in, routes, route_weight, pre_gain,
    gate_weight, up_weight, down_weight, post_gain,
    mix_out, expert_out,
    xin, sendbuf, rows_in, rows_z, part_in, part_z, sums, neigh, back, mine, theirs,
    gate_w, up_w, down_w, padded, mixed, w_all, acc, table,
    local_sem, send_a, recv_a, send_z, recv_z, send_p, recv_p, send_r, recv_r, send_t, recv_t,
    send_w, recv_w, send_o, recv_o, send_h, recv_h,
):
    i = lax.axis_index("ep")
    j = lax.axis_index("tp")
    z, c = j // 2, j % 2
    y, x = i // 4, i % 4
    p = z % 2
    here = (i, j)
    mate = (i, 2 * z + 1 - c)

    def plane(dy, dx):
        return ((y + dy) % 4) * 4 + (x + dx) % 4

    def along(dz):
        return (i, 2 * ((z + dz) % 8) + c)

    after = (jnp.where(j == 15, (i + 1) % 16, i), (j + 1) % 16)
    before = (jnp.where(j == 0, (i + 15) % 16, i), (j + 15) % 16)

    def block_row(parity, b):
        return pl.multiple_of((2 * (parity + 2 * b) + c) * 16, 16)

    loads = []

    def load(src, dst):
        copy = pltpu.make_async_copy(src, dst, local_sem.at[len(loads)])
        copy.start()
        loads.append(copy)
        return copy

    token_loads = [
        load(expert_in.at[pl.ds(block_row(1 - p, b), 16)], xin.at[pl.ds(16 * b, 16)]) for b in range(4)
    ]
    weight_loads = [
        load(gate_weight.at[c], gate_w.at[0]),
        load(up_weight.at[c], up_w.at[0]),
        load(down_weight.at[c], down_w.at[0]),
    ]
    pool_load = load(pool_in, padded.at[pl.ds(16, 512)])
    slow, fast = jnp.where(c == 0, y, x), jnp.where(c == 0, x, y)
    w_mine = slow * 4 + fast
    w_src = out_weight.at[:, pl.ds(pl.multiple_of(i * 128, 128), 128)]
    w_load = load(w_src, w_all.at[c, w_mine, z])

    bar = pltpu.get_barrier_semaphore()

    def greet(device):
        pl.semaphore_signal(bar, inc=1, device_id=device, device_id_type=MESH)

    for dy, dx in ORDER[1:]:
        for core in range(2):
            greet((plane(dy, dx), 2 * z + core))
    for dz in range(1, 8):
        greet(along(dz))
    greet(mate)
    greet((jnp.where(c == 1, after[0], before[0]), jnp.where(c == 1, after[1], before[1])))

    lane = lax.broadcasted_iota(jnp.int32, (1, 512), 1)
    expert = jnp.zeros((1, 512), jnp.int32)
    for k, (dy, dx) in enumerate(ORDER):
        expert = jnp.where(lane // 32 == k, 2 * plane(dy, dx), expert)
    expert = expert + (lane // 16) % 2
    slot_lane = lane % 16
    token = lax.broadcasted_iota(jnp.int32, (64, 64), 0)
    other = lax.broadcasted_iota(jnp.int32, (64, 64), 1)
    earlier = jnp.where((other < token) & (other // 16 == token // 16), 1.0, 0.0).astype(BF16)
    base = (lax.broadcasted_iota(jnp.int32, (64, 1), 0) // 16) * 4

    def turned(ref, column):
        block = jnp.concatenate([ref[...].astype(F32), jnp.zeros((4, 256), F32)], axis=0)
        table[:, column : column + 8] = block.T

    turned(routes, 0)
    turned(route_weight, 8)

    def selection(parity, weighted):
        rows = jnp.concatenate([table[pl.ds(block_row(parity, b), 16), :] for b in range(4)], axis=0)
        chosen, weights = rows[:, 0:4].astype(jnp.int32), rows[:, 8:12]
        hot = jnp.zeros((64, 512), F32)
        value = jnp.zeros((64, 512), F32)
        for k in range(4):
            match = chosen[:, k : k + 1] == expert
            hot = jnp.where(match, 1.0, hot)
            value = jnp.where(match, weights[:, k : k + 1], value)
        rank = jnp.dot(earlier, hot.astype(BF16), preferred_element_type=F32).astype(jnp.int32)
        taken = (rank + base) == slot_lane
        return jnp.where(taken, value if weighted else hot, 0.0)

    with phase("pack"):
        pick = selection(1 - p, False).T.astype(BF16)
        for copy in token_loads:
            copy.wait()
        tokens = xin[...].astype(F32)
        scale = lax.rsqrt(jnp.mean(tokens * tokens, axis=-1, keepdims=True) + EPS)
        normed = (tokens * scale * pre_gain[...]).astype(BF16)
        for k in range(4):
            piece = jnp.dot(pick[128 * k : 128 * k + 128], normed, preferred_element_type=F32)
            sendbuf[4 * k : 4 * k + 4] = piece.astype(BF16).reshape(4, 2, 16, 2048)

    with phase("barrier"):
        pl.semaphore_wait(bar, 39)

    def to_plane(k, core):
        dy, dx = ORDER[k]
        return remote(
            sendbuf.at[k, core], rows_in.at[k, c], send_a.at[k, core], recv_a.at[k, c],
            (plane(dy, dx), 2 * z + core),
        )

    w_z = []
    for dz in range(1, 8):
        copy = remote(w_src, w_all.at[c, w_mine, z], send_w.at[dz], recv_w.at[dz], along(dz))
        copy.start()
        w_z.append(copy)
    for k in range(1, 16):
        for core in range(2):
            to_plane(k, core).start()
    to_mate = remote(sendbuf.at[0, 1 - c], rows_in.at[0, c], send_a.at[0, 0], recv_a.at[0, 0], mate)
    to_mate.start()
    rim = remote(pool_in.at[pl.ds(496, 16)], padded.at[pl.ds(0, 16)], send_h, recv_h, after)
    rim.start()
    swaps = [
        remote(gate_weight.at[1 - c], gate_w.at[1], send_o.at[0], recv_o.at[0], mate),
        remote(up_weight.at[1 - c], up_w.at[1], send_o.at[1], recv_o.at[1], mate),
        remote(down_weight.at[1 - c], down_w.at[1], send_o.at[2], recv_o.at[2], mate),
    ]
    for copy in swaps:
        copy.start()
    rows_in[0, c] = sendbuf[0, c]

    def onward(k, core):
        return remote(
            rows_in.at[k, core], rows_z.at[k, core], send_z.at[k, core], recv_z.at[k, core],
            along(1 if core == 0 else 7),
        )

    def arrive(ks):
        for k in ks:
            if k == 0:
                to_mate.wait_recv()
            for core in range(2):
                if k:
                    remote(sendbuf.at[k, core], rows_in.at[k, core], send_a.at[k, core], recv_a.at[k, core], here).wait_recv()
                onward(k, core).start()

    def experts(source, first):
        block = source[first : first + 8].reshape(256, 2048)
        hidden = []
        for half in range(2):
            gate = jnp.dot(block, gate_w[half], preferred_element_type=F32)
            up = jnp.dot(block, up_w[half], preferred_element_type=F32)
            hidden.append(clamped_unit(gate, up).astype(BF16))
        hidden = jnp.concatenate(hidden, axis=1)
        return jnp.dot(hidden, down_w[...].reshape(512, 2048), preferred_element_type=F32)

    def partial(k, core):
        return remote(
            part_in.at[k, core], neigh.at[k, core], send_p.at[k, core], recv_p.at[k, core],
            along(1 if core == 0 else 7),
        )

    def inner(first):
        part_in[first : first + 8] = experts(rows_in, first).astype(BF16).reshape(8, 2, 16, 2048)
        for k in range(first, first + 8):
            for core in range(2):
                partial(k, core).start()

    def outer(first):
        for k in range(first, first + 8):
            for core in range(2):
                onward(k, core).wait_recv()
        part_z[first : first + 8] = experts(rows_z, first).reshape(8, 2, 16, 2048)

    def w_first():
        w_load.wait()
        for copy in w_z:
            copy.wait_recv()
        for k in range(1, 4):
            w_fast(k).start()

    def w_fast(k):
        dy, dx = jnp.where(c == 0, 0, k), jnp.where(c == 0, k, 0)
        return remote(w_all.at[c, w_mine], w_all.at[c, w_mine], send_w.at[7 + k], recv_w.at[7 + k], (plane(dy, dx), j))

    def w_slow(k):
        dy, dx = jnp.where(c == 0, k, 0), jnp.where(c == 0, 0, k)
        strip = w_all.at[c, pl.ds(slow * 4, 4)]
        return remote(strip, strip, send_w.at[10 + k], recv_w.at[10 + k], (plane(dy, dx), j))

    def w_core():
        return remote(w_all.at[c], w_all.at[c], send_w.at[0], recv_w.at[0], mate)

    def home(k, core):
        dy, dx = ORDER[k]
        return remote(
            sums.at[k, core], back.at[k, c], send_r.at[k, core], recv_r.at[k, c],
            (plane(-dy, -dx), 2 * z + core),
        )

    home_mate = remote(sums.at[0, 1 - c], back.at[0, c], send_r.at[0, 0], recv_r.at[0, 0], mate)

    def settle(ks):
        for k in ks:
            for core in range(2):
                partial(k, core).wait_recv()
            sums[k] = (part_z[k] + neigh[k].astype(F32)).astype(BF16)
            if k == 0:
                home_mate.start()
                back[0, c] = sums[0, c]
            else:
                for core in range(2):
                    home(k, core).start()

    def mixer_first():
        pool_load.wait()
        rim.wait_recv()
        number = i * 16 + j
        row = lax.broadcasted_iota(jnp.int32, (528, 1), 0)
        live = (row >= 16) | (number > 0)
        position = number * 512 + lax.broadcasted_iota(jnp.int32, (512, 1), 0)
        for g, window in enumerate(WINDOWS):
            inverse = 1.0 / jnp.minimum(position + 1, window).astype(F32)
            diffs = []
            for half in range(2):
                cols = slice(g * 256 + half * 128, g * 256 + half * 128 + 128)
                values = jnp.where(live, padded[:, cols].astype(F32), 0.0)
                total = values
                reach = 1
                while reach < window:
                    total = total + pltpu.roll(total, reach, 0)
                    reach *= 2
                diffs.append((total[16:] * inverse - values[16:]).astype(BF16))
            diff = jnp.concatenate(diffs, axis=1)
            out = jnp.dot(diff, pool_weight[g], preferred_element_type=F32)
            mixed[:, g * 256 : (g + 1) * 256] = (out * pool_gain[:, g * 256 : (g + 1) * 256]).astype(BF16)

    def w_strip():
        for k in range(1, 4):
            w_fast(k).wait_recv()
        for k in range(1, 4):
            w_slow(k).start()

    def w_half():
        for k in range(1, 4):
            w_slow(k).wait_recv()
        w_core().start()

    def weights():
        for copy in weight_loads:
            copy.wait()
        for copy in swaps:
            copy.wait_recv()

    def step(name, what, *args):
        with phase(name):
            what(*args)

    step("arrive_0", arrive, range(0, 4))
    step("w_first", w_first)
    step("arrive_4", arrive, range(4, 8))
    step("weights", weights)
    step("inner_0", inner, 0)
    step("mixer_first", mixer_first)
    step("arrive_8", arrive, range(8, 12))
    step("outer_0", outer, 0)
    step("settle_0", settle, range(0, 4))
    step("arrive_12", arrive, range(12, 16))
    step("inner_8", inner, 8)
    step("settle_4", settle, range(4, 8))
    step("w_strip", w_strip)
    step("outer_8", outer, 8)
    step("settle_8", settle, range(8, 12))
    step("settle_12", settle, range(12, 16))
    step("w_half", w_half)

    with phase("mixer_second"):
        w_core().wait_recv()
        for h in range(2):
            rows = mixed[256 * h : 256 * h + 256]
            square = jnp.zeros((256, 1), F32)
            for n in range(8):
                sides = []
                for b in (2 * n, 2 * n + 1):
                    turned = (b % 4) * 4 + b // 4
                    sides.append(
                        jnp.concatenate([w_all[core, (b, turned)[core], q] for q in range(8) for core in range(2)], axis=0)
                    )
                out = jnp.dot(rows, jnp.concatenate(sides, axis=1), preferred_element_type=F32)
                square = square + jnp.sum(out * out, axis=-1, keepdims=True)
                acc[:, 256 * n : 256 * n + 256] = out
            scale = lax.rsqrt(square * (1.0 / 2048.0) + EPS)
            mix_out[256 * h : 256 * h + 256] = (acc[...] * scale * mix_gain[...]).astype(BF16)

    weight = selection(p, True)
    high = weight.astype(BF16)
    low = (weight - high.astype(F32)).astype(BF16)
    both = jnp.concatenate([high, low], axis=0)
    with phase("back"):
        home_mate.wait_recv()
        for k in range(1, 16):
            for core in range(2):
                remote(sums.at[k, core], back.at[k, core], send_r.at[k, core], recv_r.at[k, core], here).wait_recv()
    with phase("combine"):
        total = jnp.dot(both, back[...].reshape(512, 2048), preferred_element_type=F32)
        total = total[:64] + total[64:]
        mine[...] = total.astype(BF16).reshape(4, 16, 2048)

    def spread(m):
        return remote(
            mine.at[((z + 8 - 2 * m) % 8) // 2], theirs.at[m], send_t.at[m], recv_t.at[m], along(8 - 2 * m)
        )

    with phase("reduce"):
        for m in (2, 1, 3):
            spread(m).start()
        acc[0:64] = total
        result = acc[pl.ds(pl.multiple_of((z // 2) * 16, 16), 16), :]
        for m in (1, 3, 2):
            spread(m).wait_recv()
            result = result + theirs[m].astype(F32)

    scale = lax.rsqrt(jnp.mean(result * result, axis=-1, keepdims=True) + EPS)
    expert_out[...] = (result * scale * post_gain[...]).astype(BF16)

    for copy in w_z + swaps + [rim, to_mate, home_mate, w_core()]:
        copy.wait_send()
    for k in range(1, 4):
        w_fast(k).wait_send()
        w_slow(k).wait_send()
        spread(k).wait_send()
    for k in range(16):
        for core in range(2):
            onward(k, core).wait_send()
            partial(k, core).wait_send()
            if k:
                to_plane(k, core).wait_send()
                home(k, core).wait_send()


def body(
    pool_in, pool_weight, pool_gain, out_weight, mix_gain, expert_in, routes, route_weight, pre_gain,
    gate_weight, up_weight, down_weight, post_gain,
):
    vmem = pl.BlockSpec(memory_space=pltpu.VMEM)
    hbm = pl.BlockSpec(memory_space=pl.ANY)
    dma = pltpu.SemaphoreType.DMA
    tile = (16, 2, 16, 2048)
    return pl.pallas_call(
        kernel,
        out_shape=(
            pltpu.VMEM((512, 2048), BF16),
            pltpu.VMEM((16, 2048), BF16),
        ),
        in_specs=[hbm, vmem, vmem, hbm, vmem, hbm, vmem, vmem, vmem, hbm, hbm, hbm, vmem],
        out_specs=(vmem, vmem),
        scratch_shapes=[
            pltpu.VMEM((64, 2048), BF16),
            pltpu.VMEM(tile, BF16),
            pltpu.VMEM(tile, BF16),
            pltpu.VMEM(tile, BF16),
            pltpu.VMEM(tile, BF16),
            pltpu.VMEM(tile, F32),
            pltpu.VMEM(tile, BF16),
            pltpu.VMEM(tile, BF16),
            pltpu.VMEM(tile, BF16),
            pltpu.VMEM((4, 16, 2048), BF16),
            pltpu.VMEM((4, 16, 2048), BF16),
            pltpu.VMEM((2, 2048, 256), BF16),
            pltpu.VMEM((2, 2048, 256), BF16),
            pltpu.VMEM((2, 256, 2048), BF16),
            pltpu.VMEM((528, 1024), BF16),
            pltpu.VMEM((512, 1024), BF16),
            pltpu.VMEM((2, 16, 8, 64, 128), BF16),
            pltpu.VMEM((256, 2048), F32),
            pltpu.VMEM((256, 16), F32),
            dma((9,)),
            dma((16, 2)), dma((16, 2)),
            dma((16, 2)), dma((16, 2)),
            dma((16, 2)), dma((16, 2)),
            dma((16, 2)), dma((16, 2)),
            dma((4,)), dma((4,)),
            dma((14,)), dma((14,)),
            dma((3,)), dma((3,)),
            dma, dma,
        ],
        compiler_params=pltpu.CompilerParams(
            collective_id=0, has_side_effects=True, vmem_limit_bytes=60 * 1024 * 1024
        ),
        name="mixer_experts",
    )(
        pool_in, pool_weight, pool_gain.reshape(1, -1), out_weight, mix_gain.reshape(1, -1), expert_in, routes.T,
        route_weight.T, pre_gain.reshape(1, -1), gate_weight, up_weight, down_weight, post_gain.reshape(1, -1),
    )


def solution(mesh):
    return jax.shard_map(
        body,
        mesh=mesh,
        in_specs=(
            P(("ep", "tp"), None),
            P(),
            P(),
            P("tp", None),
            P(),
            P("ep", None),
            P("ep", None),
            P("ep", None),
            P(),
            P("ep", None, "tp"),
            P("ep", None, "tp"),
            P("ep", "tp", None),
            P(),
        ),
        out_specs=(P(("ep", "tp"), None), P(("ep", "tp"), None)),
        check_vma=False,
    )
```

```python
import functools

import jax
import jax.numpy as jnp
from jax import lax
from jax.experimental import pallas as pl
from jax.experimental.pallas import tpu as pltpu
from jax.sharding import PartitionSpec as P

MESH = pl.DeviceIdType.MESH
WINDOWS = (2, 4, 8, 16)
EPS = 1e-06
LIMIT = 7.0
ALPHA = 1.702
F32 = jnp.float32
BF16 = jnp.bfloat16


phase = jax.named_scope


FIRST = (1, 3, 2, 0)
SECOND = (2, 1, 3, 0)
OWN = 3
OTHERS = (0, 1, 2)


def clamped_unit(gate, up):
    gate = jnp.minimum(gate, LIMIT)
    up = jnp.clip(up, -LIMIT, LIMIT)
    return (up + 1.0) * gate * jax.nn.sigmoid(ALPHA * gate)


def remote(src, dst, send, recv, device):
    return pltpu.make_async_remote_copy(
        src_ref=src, dst_ref=dst, send_sem=send, recv_sem=recv, device_id=device, device_id_type=MESH
    )


def kernel(
    pool_in, pool_weight, pool_gain, out_weight, mix_gain, expert_in, routes, route_weight, pre_gain,
    gate_weight, up_weight, down_weight, post_gain,
    mix_out, expert_out,
    pool_w, pool_g, mix_g, pre_g, post_g, routes_v, route_w,
    tokens, picks, picks_in, sendbuf, rows_in, rows_z, part_in, part_z, sums, neigh, back, homebuf, homes,
    mine, theirs, gate_w, up_w, down_w, padded, mixed, w_all, acc, table, xin, own,
    local_sem, send_k, recv_k, send_m, recv_m, send_f, recv_f, send_a, recv_a, send_z, recv_z, send_p, recv_p, send_r, recv_r, send_t, recv_t,
    send_w, recv_w, send_o, recv_o, send_h, recv_h,
):
    i = lax.axis_index("ep")
    j = lax.axis_index("tp")
    z, c = j // 2, j % 2
    y, x = i // 4, i % 4
    p = z % 2
    here = (i, j)
    mate = (i, 2 * z + 1 - c)

    def plane(dy, dx):
        return ((y + dy) % 4) * 4 + (x + dx) % 4

    def turn(da, db):
        return plane(jnp.where(c == 0, da, db), jnp.where(c == 0, db, da))

    def along(dz):
        return (i, 2 * ((z + dz) % 8) + c)

    after = (jnp.where(j == 15, (i + 1) % 16, i), (j + 1) % 16)
    before = (jnp.where(j == 0, (i + 15) % 16, i), (j + 15) % 16)

    bar = pltpu.get_barrier_semaphore()

    def greet(device):
        pl.semaphore_signal(bar, inc=1, device_id=device, device_id_type=MESH)

    for d in range(1, 4):
        for core in range(2):
            greet((plane(d, 0), 2 * z + core))
            greet((plane(0, d), 2 * z + core))
    for dz in range(1, 8):
        greet(along(dz))
    greet(mate)
    greet((jnp.where(c == 1, after[0], before[0]), jnp.where(c == 1, after[1], before[1])))

    def block_row(parity, b):
        return pl.multiple_of((2 * (parity + 2 * b) + c) * 16, 16)

    loads = []

    def load(src, dst):
        copy = pltpu.make_async_copy(src, dst, local_sem.at[len(loads)])
        copy.start()
        loads.append(copy)
        return copy

    table_loads = [load(routes, routes_v), load(route_weight, route_w)]
    token_loads = [
        load(expert_in.at[pl.ds(block_row(1 - p, b), 16)], xin.at[pl.ds(16 * b, 16)]) for b in range(4)
    ]
    token_loads.append(load(pre_gain, pre_g))
    weight_loads = [
        load(gate_weight.at[c], gate_w.at[0]),
        load(up_weight.at[c], up_w.at[0]),
        load(down_weight.at[c], down_w.at[0]),
    ]
    gain_loads = [load(mix_gain, mix_g), load(post_gain, post_g)]
    pool_loads = [load(pool_weight, pool_w), load(pool_gain, pool_g)]
    pool_load = load(pool_in, padded.at[pl.ds(16, 512)])
    slow, fast = jnp.where(c == 0, y, x), jnp.where(c == 0, x, y)
    w_mine = slow * 4 + fast
    w_src = out_weight.at[:, pl.ds(pl.multiple_of(i * 128, 128), 128)]
    w_load = load(w_src, w_all.at[c, w_mine, z])

    lane = lax.broadcasted_iota(jnp.int32, (1, 512), 1)
    expert = jnp.zeros((1, 512), jnp.int32)
    for k in range(16):
        expert = jnp.where(lane // 32 == k, 2 * turn(FIRST[k // 4], SECOND[k % 4]), expert)
    expert = expert + (lane // 16) % 2
    slot_lane = lane % 16
    token = lax.broadcasted_iota(jnp.int32, (64, 64), 0)
    other = lax.broadcasted_iota(jnp.int32, (64, 64), 1)
    earlier = jnp.where((other < token) & (other // 16 == token // 16), 1.0, 0.0).astype(BF16)
    base = (lax.broadcasted_iota(jnp.int32, (64, 1), 0) // 16) * 4

    def turned(ref, column):
        block = jnp.concatenate([ref[...].astype(F32), jnp.zeros((4, 256), F32)], axis=0)
        table[:, column : column + 8] = block.T

    for copy in table_loads:
        copy.wait()
    turned(routes_v, 0)
    turned(route_w, 8)

    def selection(parity, weighted):
        rows = jnp.concatenate([table[pl.ds(block_row(parity, b), 16), :] for b in range(4)], axis=0)
        chosen, weights = rows[:, 0:4].astype(jnp.int32), rows[:, 8:12]
        hot = jnp.zeros((64, 512), F32)
        value = jnp.zeros((64, 512), F32)
        for k in range(4):
            match = chosen[:, k : k + 1] == expert
            hot = jnp.where(match, 1.0, hot)
            value = jnp.where(match, weights[:, k : k + 1], value)
        rank = jnp.dot(earlier, hot.astype(BF16), preferred_element_type=F32).astype(jnp.int32)
        taken = (rank + base) == slot_lane
        return jnp.where(taken, value if weighted else hot, 0.0)

    def landed(ref, sem):
        remote(ref, ref, send_h, sem, here).wait_recv()

    def left(ref, sem):
        remote(ref, ref, sem, recv_h, here).wait_send()

    def fill(a):
        pick = picks_in[a, 0:64].astype(F32).T.astype(BF16)
        rows = jnp.dot(pick, tokens[a], preferred_element_type=F32)
        sendbuf[4 * a : 4 * a + 4] = rows.astype(BF16).reshape(4, 2, 16, 2048)

    with phase("pack"):
        pick = selection(1 - p, False).astype(BF16)
        weight = selection(p, True)
        high = weight.astype(BF16)
        low = (weight - high.astype(F32)).astype(BF16)
        for a in range(4):
            lanes = slice(128 * a, 128 * a + 128)
            picks[a] = jnp.concatenate([pick[:, lanes], high[:, lanes], low[:, lanes]], axis=0)
        picks_in[OWN] = picks[OWN]
        for copy in token_loads:
            copy.wait()
        values = xin[...].astype(F32)
        scale = lax.rsqrt(jnp.mean(values * values, axis=-1, keepdims=True) + EPS)
        tokens[OWN] = (values * scale * pre_g[...]).astype(BF16)
        fill(OWN)

    with phase("barrier"):
        pl.semaphore_wait(bar, 21)

    def to_axis(a):
        device = (turn(FIRST[a], 0), j)
        return [
            remote(tokens.at[OWN], tokens.at[a], send_k, recv_k.at[a], device),
            remote(picks.at[a], picks_in.at[a], send_m, recv_m.at[a], device),
        ]

    def to_plane(k, core):
        return remote(
            sendbuf.at[k, core], rows_in.at[k, c], send_a, recv_a.at[k],
            (turn(0, SECOND[k % 4]), 2 * z + core),
        )

    def to_mate(k):
        return remote(sendbuf.at[k, 1 - c], rows_in.at[k, c], send_a, recv_a.at[k], mate)

    def pack(a):
        if a != OWN:
            for copy in to_axis(a):
                copy.wait_recv()
            fill(a)
        to_mate(4 * a + OWN).start()
        for b in OTHERS:
            for core in range(2):
                to_plane(4 * a + b, core).start()
        rows_in[4 * a + OWN, c] = sendbuf[4 * a + OWN, c]

    def axis():
        for a in OTHERS:
            for copy in to_axis(a):
                copy.start()

    def w_begin():
        for copy in w_z:
            copy.start()

    w_z = []
    for dz in range(1, 8):
        copy = remote(w_src, w_all.at[c, w_mine, z], send_w.at[0], recv_w.at[0], along(dz))
        w_z.append(copy)
    rim = remote(pool_in.at[pl.ds(496, 16)], padded.at[pl.ds(0, 16)], send_h, recv_h, after)
    swaps = [
        remote(gate_weight.at[1 - c], gate_w.at[1], send_o.at[0], recv_o.at[0], mate),
        remote(up_weight.at[1 - c], up_w.at[1], send_o.at[1], recv_o.at[1], mate),
        remote(down_weight.at[1 - c], down_w.at[1], send_o.at[2], recv_o.at[2], mate),
    ]

    def onward(k, core):
        return remote(
            rows_in.at[k, core], rows_z.at[k, core], send_z, recv_z.at[k // 8],
            along(1 if core == 0 else 7),
        )

    def arrive(ks):
        for k in ks:
            if k % 4 != OWN:
                landed(rows_in.at[k], recv_a.at[k])
            else:
                landed(rows_in.at[k, 1 - c], recv_a.at[k])
            for core in range(2):
                onward(k, core).start()

    def experts(source, first, count):
        block = source[first : first + count].reshape(32 * count, 2048)
        hidden = []
        for half in range(2):
            gate = jnp.dot(block, gate_w[half], preferred_element_type=F32)
            up = jnp.dot(block, up_w[half], preferred_element_type=F32)
            hidden.append(clamped_unit(gate, up).astype(BF16))
        hidden = jnp.concatenate(hidden, axis=1)
        return jnp.dot(hidden, down_w[...].reshape(512, 2048), preferred_element_type=F32)

    def partial(k, core):
        return remote(
            part_in.at[k, core], neigh.at[k, core], send_p, recv_p.at[k],
            along(1 if core == 0 else 7),
        )

    def inner(first, count):
        part = experts(rows_in, first, count)
        part_in[first : first + count] = part.astype(BF16).reshape(count, 2, 16, 2048)
        for k in range(first, first + count):
            for core in range(2):
                partial(k, core).start()

    def outer(first, count):
        landed(rows_z.at[pl.ds(first, count)], recv_z.at[first // 8])
        part_z[first : first + count] = experts(rows_z, first, count).reshape(count, 2, 16, 2048)

    def w_first():
        w_load.wait()
        landed(w_all.at[c, w_mine, pl.ds(0, 7)], recv_w.at[0])
        for k in range(1, 4):
            w_fast(k).start()

    def w_fast(k):
        dy, dx = jnp.where(c == 0, 0, k), jnp.where(c == 0, k, 0)
        return remote(w_all.at[c, w_mine], w_all.at[c, w_mine], send_w.at[1], recv_w.at[1], (plane(dy, dx), j))

    def w_slow(k):
        dy, dx = jnp.where(c == 0, k, 0), jnp.where(c == 0, 0, k)
        strip = w_all.at[c, pl.ds(slow * 4, 4)]
        return remote(strip, strip, send_w.at[2], recv_w.at[2], (plane(dy, dx), j))

    def w_core():
        return remote(w_all.at[c], w_all.at[c], send_w.at[3], recv_w.at[3], mate)

    def home(k, core):
        step_back = -SECOND[k % 4]
        there = plane(0, step_back) if core == 0 else plane(step_back, 0)
        return remote(
            sums.at[k, core], back.at[k, c], send_r, recv_r.at[k // 4], (there, 2 * z + core)
        )

    def home_mate(k):
        return remote(sums.at[k, 1 - c], back.at[k, c], send_r, recv_r.at[k // 4], mate)

    def settle(ks):
        for k in ks:
            landed(neigh.at[k], recv_p.at[k])
            sums[k] = (part_z[k] + neigh[k].astype(F32)).astype(BF16)
            if k % 4 != OWN:
                for core in range(2):
                    home(k, core).start()
            else:
                home_mate(k).start()
                back[k, c] = sums[k, c]

    def to_home(a):
        return remote(homebuf.at[a], homes.at[a], send_f, recv_f.at[a], (turn(-FIRST[a], 0), j))

    def combine(a):
        landed(back.at[pl.ds(0, 7), 0], recv_r.at[a])
        rows = back[4 * a : 4 * a + 4].reshape(128, 2048)
        both = jnp.dot(picks_in[a, 64:192], rows, preferred_element_type=F32)
        total = both[:64] + both[64:]
        if a != OWN:
            homebuf[a] = total.astype(BF16)
            to_home(a).start()
        else:
            own[...] = total

    def mixer_first():
        for copy in pool_loads + [pool_load]:
            copy.wait()
        rim.wait_recv()
        number = i * 16 + j
        row = lax.broadcasted_iota(jnp.int32, (528, 1), 0)
        live = (row >= 16) | (number > 0)
        position = number * 512 + lax.broadcasted_iota(jnp.int32, (512, 1), 0)
        for g, window in enumerate(WINDOWS):
            inverse = 1.0 / jnp.minimum(position + 1, window).astype(F32)
            diffs = []
            for half in range(2):
                cols = slice(g * 256 + half * 128, g * 256 + half * 128 + 128)
                values = jnp.where(live, padded[:, cols].astype(F32), 0.0)
                total = values
                reach = 1
                while reach < window:
                    total = total + pltpu.roll(total, reach, 0)
                    reach *= 2
                diffs.append((total[16:] * inverse - values[16:]).astype(BF16))
            diff = jnp.concatenate(diffs, axis=1)
            out = jnp.dot(diff, pool_w[g], preferred_element_type=F32)
            mixed[:, g * 256 : (g + 1) * 256] = (out * pool_g[:, g * 256 : (g + 1) * 256]).astype(BF16)

    def w_strip():
        landed(w_all.at[c, pl.ds(0, 3)], recv_w.at[1])
        for k in range(1, 4):
            w_slow(k).start()

    def w_half():
        landed(w_all.at[c, pl.ds(0, 12)], recv_w.at[2])
        w_core().start()

    def weights():
        for copy in weight_loads:
            copy.wait()
        for copy in swaps:
            copy.wait_recv()

    def swap(n):
        swaps[n].start()

    def rim_begin():
        rim.start()

    def step(name, what, *args):
        with phase(name):
            what(*args)

    def mixer_second():
        for copy in gain_loads:
            copy.wait()
        w_core().wait_recv()
        for h in range(2):
            rows = mixed[256 * h : 256 * h + 256]
            square = jnp.zeros((256, 1), F32)
            for n in range(8):
                sides = []
                for b in (2 * n, 2 * n + 1):
                    turned = (b % 4) * 4 + b // 4
                    sides.append(
                        jnp.concatenate([w_all[core, (b, turned)[core], q] for q in range(8) for core in range(2)], axis=0)
                    )
                out = jnp.dot(rows, jnp.concatenate(sides, axis=1), preferred_element_type=F32)
                square = square + jnp.sum(out * out, axis=-1, keepdims=True)
                acc[:, 256 * n : 256 * n + 256] = out
            scale = lax.rsqrt(square * (1.0 / 2048.0) + EPS)
            mix_out[256 * h : 256 * h + 256] = (acc[...] * scale * mix_g[...]).astype(BF16)

    step("00_w_begin", w_begin)
    step("01_axis", axis)
    step("02_pack_3", pack, 3)
    step("03_rim_begin", rim_begin)
    step("04_arrive_15", arrive, (15,))
    step("05_swap_0", swap, 0)
    step("06_arrive_12_13_14", arrive, (12,13,14))
    step("07_pack_0", pack, 0)
    step("08_swap_1", swap, 1)
    step("09_pack_1", pack, 1)
    step("10_arrive_3_0_1_2", arrive, (3,0,1,2))
    step("11_swap_2", swap, 2)
    step("12_pack_2", pack, 2)
    step("13_w_first", w_first)
    step("14_arrive_7_4_5_6", arrive, (7,4,5,6))
    step("15_weights", weights)
    step("16_inner_0_8", inner, 0,8)
    step("17_arrive_11_8_9_10", arrive, (11,8,9,10))
    step("18_mixer_first", mixer_first)
    step("19_w_strip", w_strip)
    step("20_inner_8_8", inner, 8,8)
    step("21_outer_0_8", outer, 0,8)
    step("22_settle_0_1_2_3", settle, (0,1,2,3))
    step("23_settle_4_5_6_7", settle, (4,5,6,7))
    step("24_outer_8_8", outer, 8,8)
    step("25_combine_0", combine, 0)
    step("26_combine_1", combine, 1)
    step("27_w_half", w_half)
    step("28_settle_8_9_10_11", settle, (8,9,10,11))
    step("29_settle_12_13_14_15", settle, (12,13,14,15))
    step("30_combine_2", combine, 2)
    step("31_mixer_second", mixer_second)
    step("32_combine_3", combine, 3)
    with phase("home"):
        total = own[...]
        for a in OTHERS:
            to_home(a).wait_recv()
            total = total + homes[a].astype(F32)
    mine[...] = total.astype(BF16).reshape(4, 16, 2048)

    def spread(m):
        return remote(
            mine.at[((z + 8 - 2 * m) % 8) // 2], theirs.at[m], send_t, recv_t.at[m], along(8 - 2 * m)
        )

    with phase("reduce"):
        for m in (2, 1, 3):
            spread(m).start()
        own[...] = total
        result = own[pl.ds(pl.multiple_of((z // 2) * 16, 16), 16), :]
        for m in (1, 3, 2):
            spread(m).wait_recv()
            result = result + theirs[m].astype(F32)

    with phase("norm"):
        scale = lax.rsqrt(jnp.mean(result * result, axis=-1, keepdims=True) + EPS)
        expert_out[...] = (result * scale * post_g[...]).astype(BF16)

    with phase("drain"):
        for copy in swaps + [rim, w_core()]:
            copy.wait_send()
        left(tokens.at[pl.ds(0, 3)], send_k)
        left(picks.at[pl.ds(0, 3)], send_m)
        left(homebuf.at[pl.ds(0, 3)], send_f)
        left(mine.at[pl.ds(0, 3)], send_t)
        left(w_all.at[c, w_mine, pl.ds(0, 7)], send_w.at[0])
        left(w_all.at[c, pl.ds(0, 3)], send_w.at[1])
        left(w_all.at[c, pl.ds(0, 12)], send_w.at[2])
        left(sendbuf.at[pl.ds(0, 14)], send_a)
        left(rows_in, send_z)
        left(part_in, send_p)
        left(sums.at[pl.ds(0, 14)], send_r)


def body(
    pool_in, pool_weight, pool_gain, out_weight, mix_gain, expert_in, routes, route_weight, pre_gain,
    gate_weight, up_weight, down_weight, post_gain,
):
    vmem = pl.BlockSpec(memory_space=pltpu.VMEM)
    hbm = pl.BlockSpec(memory_space=pl.ANY)
    dma = pltpu.SemaphoreType.DMA
    tile = (16, 2, 16, 2048)
    return pl.pallas_call(
        kernel,
        out_shape=(
            pltpu.VMEM((512, 2048), BF16),
            pltpu.VMEM((16, 2048), BF16),
        ),
        in_specs=[hbm] * 13,
        out_specs=(vmem, vmem),
        scratch_shapes=[
            pltpu.VMEM((4, 256, 256), BF16),
            pltpu.VMEM((1, 1024), F32),
            pltpu.VMEM((1, 2048), F32),
            pltpu.VMEM((1, 2048), F32),
            pltpu.VMEM((1, 2048), F32),
            pltpu.VMEM((4, 256), jnp.int32),
            pltpu.VMEM((4, 256), F32),
            pltpu.VMEM((4, 64, 2048), BF16),
            pltpu.VMEM((4, 192, 128), BF16),
            pltpu.VMEM((4, 192, 128), BF16),
            pltpu.VMEM(tile, BF16),
            pltpu.VMEM(tile, BF16),
            pltpu.VMEM(tile, BF16),
            pltpu.VMEM(tile, BF16),
            pltpu.VMEM(tile, F32),
            pltpu.VMEM(tile, BF16),
            pltpu.VMEM(tile, BF16),
            pltpu.VMEM(tile, BF16),
            pltpu.VMEM((4, 64, 2048), BF16),
            pltpu.VMEM((4, 64, 2048), BF16),
            pltpu.VMEM((4, 16, 2048), BF16),
            pltpu.VMEM((4, 16, 2048), BF16),
            pltpu.VMEM((2, 2048, 256), BF16),
            pltpu.VMEM((2, 2048, 256), BF16),
            pltpu.VMEM((2, 256, 2048), BF16),
            pltpu.VMEM((528, 1024), BF16),
            pltpu.VMEM((512, 1024), BF16),
            pltpu.VMEM((2, 16, 8, 64, 128), BF16),
            pltpu.VMEM((256, 2048), F32),
            pltpu.VMEM((256, 16), F32),
            pltpu.VMEM((64, 2048), BF16),
            pltpu.VMEM((64, 2048), F32),
            dma((16,)),
            dma, dma((4,)),
            dma, dma((4,)),
            dma, dma((4,)),
            dma, dma((16,)),
            dma, dma((2,)),
            dma, dma((16,)),
            dma, dma((4,)),
            dma, dma((4,)),
            dma((4,)), dma((4,)),
            dma((3,)), dma((3,)),
            dma, dma,
        ],
        compiler_params=pltpu.CompilerParams(
            collective_id=0, has_side_effects=True, vmem_limit_bytes=60 * 1024 * 1024
        ),
        name="mixer_experts",
    )(
        pool_in, pool_weight, pool_gain.reshape(1, -1), out_weight, mix_gain.reshape(1, -1), expert_in, routes.T,
        route_weight.T, pre_gain.reshape(1, -1), gate_weight, up_weight, down_weight, post_gain.reshape(1, -1),
    )


def solution(mesh):
    return jax.shard_map(
        body,
        mesh=mesh,
        in_specs=(
            P(("ep", "tp"), None),
            P(),
            P(),
            P("tp", None),
            P(),
            P("ep", None),
            P("ep", None),
            P("ep", None),
            P(),
            P("ep", None, "tp"),
            P("ep", None, "tp"),
            P("ep", "tp", None),
            P(),
        ),
        out_specs=(P(("ep", "tp"), None), P(("ep", "tp"), None)),
        check_vma=False,
    )
```

```python
import functools

import jax
import jax.numpy as jnp
from jax import lax
from jax.experimental import pallas as pl
from jax.experimental.pallas import tpu as pltpu
from jax.sharding import PartitionSpec as P

MESH = pl.DeviceIdType.MESH
WINDOWS = (2, 4, 8, 16)
EPS = 1e-06
LIMIT = 7.0
ALPHA = 1.702
F32 = jnp.float32
BF16 = jnp.bfloat16


phase = jax.named_scope


FIRST = (1, 3, 2, 0)
SECOND = (2, 1, 3, 0)
OWN = 3
OTHERS = (0, 1, 2)
PARTS = 2


def clamped_unit(gate, up):
    gate = jnp.minimum(gate, LIMIT)
    up = jnp.clip(up, -LIMIT, LIMIT)
    return (up + 1.0) * gate * jax.nn.sigmoid(ALPHA * gate)


def remote(src, dst, send, recv, device):
    return pltpu.make_async_remote_copy(
        src_ref=src, dst_ref=dst, send_sem=send, recv_sem=recv, device_id=device, device_id_type=MESH
    )


def kernel(
    pool_in, pool_weight, pool_gain, out_weight, mix_gain, expert_in, routes, route_weight, pre_gain,
    gate_weight, up_weight, down_weight, post_gain,
    mix_out, expert_out,
    pool_w, pool_g, mix_g, pre_g, post_g, routes_v, route_w,
    tokens, picks, picks_in, sendbuf, rows_in, rows_z, part_in, part_z, sums, neigh, back, homebuf, homes,
    mine, theirs, gate_w, up_w, down_w, padded, mixed, w_all, acc, table, xin, own,
    local_sem, send_k, recv_k, send_m, recv_m, send_f, recv_f, send_a, recv_a, send_z, recv_z, send_p, recv_p, send_r, recv_r, send_t, recv_t,
    send_w, recv_w, send_o, recv_o, send_h, recv_h,
):
    i = lax.axis_index("ep")
    j = lax.axis_index("tp")
    z, c = j // 2, j % 2
    y, x = i // 4, i % 4
    p = z % 2
    here = (i, j)
    mate = (i, 2 * z + 1 - c)

    def plane(dy, dx):
        return ((y + dy) % 4) * 4 + (x + dx) % 4

    def turn(da, db):
        return plane(jnp.where(c == 0, da, db), jnp.where(c == 0, db, da))

    def along(dz):
        return (i, 2 * ((z + dz) % 8) + c)

    after = (jnp.where(j == 15, (i + 1) % 16, i), (j + 1) % 16)
    before = (jnp.where(j == 0, (i + 15) % 16, i), (j + 15) % 16)

    bar = pltpu.get_barrier_semaphore()

    def greet(device):
        pl.semaphore_signal(bar, inc=1, device_id=device, device_id_type=MESH)

    for d in range(1, 4):
        for core in range(2):
            greet((plane(d, 0), 2 * z + core))
            greet((plane(0, d), 2 * z + core))
    for dz in range(1, 8):
        greet(along(dz))
    greet(mate)
    greet((jnp.where(c == 1, after[0], before[0]), jnp.where(c == 1, after[1], before[1])))

    def block_row(parity, b):
        return pl.multiple_of((2 * (parity + 2 * b) + c) * 16, 16)

    loads = []

    def load(src, dst):
        copy = pltpu.make_async_copy(src, dst, local_sem.at[len(loads)])
        copy.start()
        loads.append(copy)
        return copy

    table_loads = [load(routes, routes_v), load(route_weight, route_w)]
    token_loads = [
        load(expert_in.at[pl.ds(block_row(1 - p, b), 16)], xin.at[pl.ds(16 * b, 16)]) for b in range(4)
    ]
    token_loads.append(load(pre_gain, pre_g))
    weight_loads = [
        load(gate_weight.at[c], gate_w.at[0]),
        load(up_weight.at[c], up_w.at[0]),
        load(down_weight.at[c], down_w.at[0]),
    ]
    gain_loads = [load(mix_gain, mix_g), load(post_gain, post_g)]
    pool_loads = [load(pool_weight, pool_w), load(pool_gain, pool_g)]
    pool_load = load(pool_in, padded.at[pl.ds(16, 512)])
    slow, fast = jnp.where(c == 0, y, x), jnp.where(c == 0, x, y)
    w_mine = slow * 4 + fast
    w_src = out_weight.at[:, pl.ds(pl.multiple_of(i * 128, 128), 128)]
    w_load = load(w_src, w_all.at[c, w_mine, z])

    lane = lax.broadcasted_iota(jnp.int32, (1, 512), 1)
    expert = jnp.zeros((1, 512), jnp.int32)
    for k in range(16):
        expert = jnp.where(lane // 32 == k, 2 * turn(FIRST[k // 4], SECOND[k % 4]), expert)
    expert = expert + (lane // 16) % 2
    slot_lane = lane % 16
    token = lax.broadcasted_iota(jnp.int32, (64, 64), 0)
    other = lax.broadcasted_iota(jnp.int32, (64, 64), 1)
    earlier = jnp.where((other < token) & (other // 16 == token // 16), 1.0, 0.0).astype(BF16)
    base = (lax.broadcasted_iota(jnp.int32, (64, 1), 0) // 16) * 4

    def turned(ref, column):
        block = jnp.concatenate([ref[...].astype(F32), jnp.zeros((4, 256), F32)], axis=0)
        table[:, column : column + 8] = block.T

    for copy in table_loads:
        copy.wait()
    turned(routes_v, 0)
    turned(route_w, 8)

    def selection(parity, weighted):
        rows = jnp.concatenate([table[pl.ds(block_row(parity, b), 16), :] for b in range(4)], axis=0)
        chosen, weights = rows[:, 0:4].astype(jnp.int32), rows[:, 8:12]
        hot = jnp.zeros((64, 512), F32)
        value = jnp.zeros((64, 512), F32)
        for k in range(4):
            match = chosen[:, k : k + 1] == expert
            hot = jnp.where(match, 1.0, hot)
            value = jnp.where(match, weights[:, k : k + 1], value)
        rank = jnp.dot(earlier, hot.astype(BF16), preferred_element_type=F32).astype(jnp.int32)
        taken = (rank + base) == slot_lane
        return jnp.where(taken, value if weighted else hot, 0.0)

    def landed(ref, sem):
        remote(ref, ref, send_h, sem, here).wait_recv()

    def left(ref, sem):
        remote(ref, ref, sem, recv_h, here).wait_send()

    def fill(a):
        pick = picks_in[a, 0:64].astype(F32).T.astype(BF16)
        rows = jnp.dot(pick, tokens[a], preferred_element_type=F32)
        sendbuf[4 * a : 4 * a + 4] = rows.astype(BF16).reshape(4, 2, 16, 2048)

    with phase("pack"):
        pick = selection(1 - p, False).astype(BF16)
        weight = selection(p, True)
        high = weight.astype(BF16)
        low = (weight - high.astype(F32)).astype(BF16)
        for a in range(4):
            lanes = slice(128 * a, 128 * a + 128)
            picks[a] = jnp.concatenate([pick[:, lanes], high[:, lanes], low[:, lanes]], axis=0)
        picks_in[OWN] = picks[OWN]
        for copy in token_loads:
            copy.wait()
        values = xin[...].astype(F32)
        scale = lax.rsqrt(jnp.mean(values * values, axis=-1, keepdims=True) + EPS)
        tokens[OWN] = (values * scale * pre_g[...]).astype(BF16)
        fill(OWN)

    with phase("barrier"):
        pl.semaphore_wait(bar, 21)

    def to_axis(a):
        device = (turn(FIRST[a], 0), j)
        return [
            remote(tokens.at[OWN], tokens.at[a], send_k, recv_k.at[a], device),
            remote(picks.at[a], picks_in.at[a], send_m, recv_m.at[a], device),
        ]

    def to_plane(k, core):
        return remote(
            sendbuf.at[k, core], rows_in.at[k, c], send_a, recv_a.at[k],
            (turn(0, SECOND[k % 4]), 2 * z + core),
        )

    def to_mate(k):
        return remote(sendbuf.at[k, 1 - c], rows_in.at[k, c], send_a, recv_a.at[k], mate)

    def pack(a):
        if a != OWN:
            for copy in to_axis(a):
                copy.wait_recv()
            fill(a)
        to_mate(4 * a + OWN).start()
        for b in OTHERS:
            for core in range(2):
                to_plane(4 * a + b, core).start()
        rows_in[4 * a + OWN, c] = sendbuf[4 * a + OWN, c]

    def axis():
        for a in OTHERS:
            for copy in to_axis(a):
                copy.start()

    def w_begin():
        for copy in w_z:
            copy.start()

    w_z = []
    for dz in range(1, 8):
        copy = remote(w_src, w_all.at[c, w_mine, z], send_w.at[0], recv_w.at[0], along(dz))
        w_z.append(copy)
    rim = remote(pool_in.at[pl.ds(496, 16)], padded.at[pl.ds(0, 16)], send_h, recv_h, after)
    swaps = [
        remote(gate_weight.at[1 - c], gate_w.at[1], send_o.at[0], recv_o.at[0], mate),
        remote(up_weight.at[1 - c], up_w.at[1], send_o.at[1], recv_o.at[1], mate),
        remote(down_weight.at[1 - c], down_w.at[1], send_o.at[2], recv_o.at[2], mate),
    ]

    def onward(k, core):
        return remote(
            rows_in.at[k, core], rows_z.at[k, core], send_z, recv_z.at[k // 8],
            along(1 if core == 0 else 7),
        )

    def arrive(ks):
        for k in ks:
            if k % 4 != OWN:
                landed(rows_in.at[k], recv_a.at[k])
            else:
                landed(rows_in.at[k, 1 - c], recv_a.at[k])
            for core in range(2):
                onward(k, core).start()

    def experts(source, first, count):
        block = source[first : first + count].reshape(32 * count, 2048)
        hidden = []
        for half in range(2):
            gate = jnp.dot(block, gate_w[half], preferred_element_type=F32)
            up = jnp.dot(block, up_w[half], preferred_element_type=F32)
            hidden.append(clamped_unit(gate, up).astype(BF16))
        hidden = jnp.concatenate(hidden, axis=1)
        return jnp.dot(hidden, down_w[...].reshape(512, 2048), preferred_element_type=F32)

    def partial(k, core):
        return remote(
            part_in.at[k, core], neigh.at[k, core], send_p, recv_p.at[k],
            along(1 if core == 0 else 7),
        )

    def inner(first, count):
        part = experts(rows_in, first, count)
        part_in[first : first + count] = part.astype(BF16).reshape(count, 2, 16, 2048)
        for k in range(first, first + count):
            for core in range(2):
                partial(k, core).start()

    def outer(first, count):
        landed(rows_z.at[pl.ds(first, count)], recv_z.at[first // 8])
        part_z[first : first + count] = experts(rows_z, first, count).reshape(count, 2, 16, 2048)

    def w_first():
        w_load.wait()
        landed(w_all.at[c, w_mine, pl.ds(0, 7)], recv_w.at[0])
        for k in range(1, 4):
            w_fast(k).start()

    def w_fast(k):
        dy, dx = jnp.where(c == 0, 0, k), jnp.where(c == 0, k, 0)
        return remote(w_all.at[c, w_mine], w_all.at[c, w_mine], send_w.at[1], recv_w.at[1], (plane(dy, dx), j))

    def w_slow(k):
        dy, dx = jnp.where(c == 0, k, 0), jnp.where(c == 0, 0, k)
        strip = w_all.at[c, pl.ds(slow * 4, 4)]
        return remote(strip, strip, send_w.at[2], recv_w.at[2], (plane(dy, dx), j))

    def w_core():
        return remote(w_all.at[c], w_all.at[c], send_w.at[3], recv_w.at[3], mate)

    def home(k, core):
        step_back = -SECOND[k % 4]
        there = plane(0, step_back) if core == 0 else plane(step_back, 0)
        return remote(
            sums.at[k, core], back.at[k, c], send_r, recv_r.at[k // 4], (there, 2 * z + core)
        )

    def home_mate(k):
        return remote(sums.at[k, 1 - c], back.at[k, c], send_r, recv_r.at[k // 4], mate)

    def settle(ks):
        for k in ks:
            landed(neigh.at[k], recv_p.at[k])
            sums[k] = (part_z[k] + neigh[k].astype(F32)).astype(BF16)
            if k % 4 != OWN:
                for core in range(2):
                    home(k, core).start()
            else:
                home_mate(k).start()
                back[k, c] = sums[k, c]

    def to_home(a):
        return remote(homebuf.at[a], homes.at[a], send_f, recv_f.at[a], (turn(-FIRST[a], 0), j))

    def cut(h):
        return pl.ds(h * (2048 // PARTS), 2048 // PARTS)

    def to_home_last(h):
        part = (2, slice(None), cut(h))
        return remote(homebuf.at[part], homes.at[part], send_f, recv_f.at[2 + h], (turn(-FIRST[2], 0), j))

    def combine(a):
        landed(back.at[pl.ds(0, 7), 0], recv_r.at[a])
        rows = back[4 * a : 4 * a + 4].reshape(128, 2048)
        both = jnp.dot(picks_in[a, 64:192], rows, preferred_element_type=F32)
        total = both[:64] + both[64:]
        if a != OWN:
            homebuf[a] = total.astype(BF16)
            for copy in [to_home_last(h) for h in range(PARTS)] if a == 2 else [to_home(a)]:
                copy.start()
        else:
            own[...] = total

    def mixer_first():
        for copy in pool_loads + [pool_load]:
            copy.wait()
        rim.wait_recv()
        number = i * 16 + j
        row = lax.broadcasted_iota(jnp.int32, (528, 1), 0)
        live = (row >= 16) | (number > 0)
        position = number * 512 + lax.broadcasted_iota(jnp.int32, (512, 1), 0)
        for g, window in enumerate(WINDOWS):
            inverse = 1.0 / jnp.minimum(position + 1, window).astype(F32)
            diffs = []
            for half in range(2):
                cols = slice(g * 256 + half * 128, g * 256 + half * 128 + 128)
                values = jnp.where(live, padded[:, cols].astype(F32), 0.0)
                total = values
                reach = 1
                while reach < window:
                    total = total + pltpu.roll(total, reach, 0)
                    reach *= 2
                diffs.append((total[16:] * inverse - values[16:]).astype(BF16))
            diff = jnp.concatenate(diffs, axis=1)
            out = jnp.dot(diff, pool_w[g], preferred_element_type=F32)
            mixed[:, g * 256 : (g + 1) * 256] = (out * pool_g[:, g * 256 : (g + 1) * 256]).astype(BF16)

    def w_strip():
        landed(w_all.at[c, pl.ds(0, 3)], recv_w.at[1])
        for k in range(1, 4):
            w_slow(k).start()

    def w_half():
        landed(w_all.at[c, pl.ds(0, 12)], recv_w.at[2])
        w_core().start()

    def weights():
        for copy in weight_loads:
            copy.wait()
        for copy in swaps:
            copy.wait_recv()

    def swap(n):
        swaps[n].start()

    def rim_begin():
        rim.start()

    def step(name, what, *args):
        with phase(name):
            what(*args)

    def mixer_second():
        for copy in gain_loads:
            copy.wait()
        w_core().wait_recv()
        for h in range(2):
            rows = mixed[256 * h : 256 * h + 256]
            square = jnp.zeros((256, 1), F32)
            for n in range(8):
                sides = []
                for b in (2 * n, 2 * n + 1):
                    turned = (b % 4) * 4 + b // 4
                    sides.append(
                        jnp.concatenate([w_all[core, (b, turned)[core], q] for q in range(8) for core in range(2)], axis=0)
                    )
                out = jnp.dot(rows, jnp.concatenate(sides, axis=1), preferred_element_type=F32)
                square = square + jnp.sum(out * out, axis=-1, keepdims=True)
                acc[:, 256 * n : 256 * n + 256] = out
            scale = lax.rsqrt(square * (1.0 / 2048.0) + EPS)
            mix_out[256 * h : 256 * h + 256] = (acc[...] * scale * mix_g[...]).astype(BF16)

    step("00_w_begin", w_begin)
    step("01_axis", axis)
    step("02_pack_3", pack, 3)
    step("03_rim_begin", rim_begin)
    step("04_arrive_15", arrive, (15,))
    step("05_swap_0", swap, 0)
    step("06_arrive_12_13_14", arrive, (12,13,14))
    step("07_pack_0", pack, 0)
    step("08_swap_1", swap, 1)
    step("09_pack_1", pack, 1)
    step("10_arrive_3_0_1_2", arrive, (3,0,1,2))
    step("11_swap_2", swap, 2)
    step("12_pack_2", pack, 2)
    step("13_w_first", w_first)
    step("14_arrive_7_4_5_6", arrive, (7,4,5,6))
    step("15_weights", weights)
    step("16_inner_0_8", inner, 0,8)
    step("17_arrive_11_8_9_10", arrive, (11,8,9,10))
    step("18_mixer_first", mixer_first)
    step("19_w_strip", w_strip)
    step("20_inner_8_8", inner, 8,8)
    step("21_outer_0_8", outer, 0,8)
    step("22_settle_0_1_2_3", settle, (0,1,2,3))
    step("23_settle_4_5_6_7", settle, (4,5,6,7))
    step("24_outer_8_8", outer, 8,8)
    step("25_combine_0", combine, 0)
    step("26_combine_1", combine, 1)
    step("27_w_half", w_half)
    step("28_settle_8_9_10_11", settle, (8,9,10,11))
    step("29_settle_12_13_14", settle, (12,13,14))
    step("30_combine_2", combine, 2)
    step("31_settle_15", settle, (15,))
    step("32_combine_3", combine, 3)
    def spread(m, h):
        return remote(
            mine.at[((z + 8 - 2 * m) % 8) // 2, :, cut(h)], theirs.at[m, :, cut(h)], send_t, recv_t.at[m, h],
            along(8 - 2 * m),
        )

    with phase("home"):
        total = own[...]
        for a in range(2):
            to_home(a).wait_recv()
            total = total + homes[a].astype(F32)
        own[...] = total
        for h in range(PARTS):
            to_home_last(h).wait_recv()
            part = own[:, cut(h)] + homes[2, :, cut(h)].astype(F32)
            mine[:, :, cut(h)] = part.astype(BF16).reshape(4, 16, 2048 // PARTS)
            for m in (2, 1, 3):
                spread(m, h).start()
            own[:, cut(h)] = part

    with phase("reduce"):
        mixer_second()
        result = own[pl.ds(pl.multiple_of((z // 2) * 16, 16), 16), :]
        for m in (1, 3, 2):
            for h in range(PARTS):
                spread(m, h).wait_recv()
            result = result + theirs[m].astype(F32)

    with phase("norm"):
        scale = lax.rsqrt(jnp.mean(result * result, axis=-1, keepdims=True) + EPS)
        expert_out[...] = (result * scale * post_g[...]).astype(BF16)

    with phase("drain"):
        for copy in swaps + [rim, w_core()]:
            copy.wait_send()
        left(tokens.at[pl.ds(0, 3)], send_k)
        left(picks.at[pl.ds(0, 3)], send_m)
        left(homebuf.at[pl.ds(0, 3)], send_f)
        left(mine.at[pl.ds(0, 3)], send_t)
        left(w_all.at[c, w_mine, pl.ds(0, 7)], send_w.at[0])
        left(w_all.at[c, pl.ds(0, 3)], send_w.at[1])
        left(w_all.at[c, pl.ds(0, 12)], send_w.at[2])
        left(sendbuf.at[pl.ds(0, 14)], send_a)
        left(rows_in, send_z)
        left(part_in, send_p)
        left(sums.at[pl.ds(0, 14)], send_r)


def body(
    pool_in, pool_weight, pool_gain, out_weight, mix_gain, expert_in, routes, route_weight, pre_gain,
    gate_weight, up_weight, down_weight, post_gain,
):
    vmem = pl.BlockSpec(memory_space=pltpu.VMEM)
    hbm = pl.BlockSpec(memory_space=pl.ANY)
    dma = pltpu.SemaphoreType.DMA
    tile = (16, 2, 16, 2048)
    return pl.pallas_call(
        kernel,
        out_shape=(
            pltpu.VMEM((512, 2048), BF16),
            pltpu.VMEM((16, 2048), BF16),
        ),
        in_specs=[hbm] * 13,
        out_specs=(vmem, vmem),
        scratch_shapes=[
            pltpu.VMEM((4, 256, 256), BF16),
            pltpu.VMEM((1, 1024), F32),
            pltpu.VMEM((1, 2048), F32),
            pltpu.VMEM((1, 2048), F32),
            pltpu.VMEM((1, 2048), F32),
            pltpu.VMEM((4, 256), jnp.int32),
            pltpu.VMEM((4, 256), F32),
            pltpu.VMEM((4, 64, 2048), BF16),
            pltpu.VMEM((4, 192, 128), BF16),
            pltpu.VMEM((4, 192, 128), BF16),
            pltpu.VMEM(tile, BF16),
            pltpu.VMEM(tile, BF16),
            pltpu.VMEM(tile, BF16),
            pltpu.VMEM(tile, BF16),
            pltpu.VMEM(tile, F32),
            pltpu.VMEM(tile, BF16),
            pltpu.VMEM(tile, BF16),
            pltpu.VMEM(tile, BF16),
            pltpu.VMEM((4, 64, 2048), BF16),
            pltpu.VMEM((4, 64, 2048), BF16),
            pltpu.VMEM((4, 16, 2048), BF16),
            pltpu.VMEM((4, 16, 2048), BF16),
            pltpu.VMEM((2, 2048, 256), BF16),
            pltpu.VMEM((2, 2048, 256), BF16),
            pltpu.VMEM((2, 256, 2048), BF16),
            pltpu.VMEM((528, 1024), BF16),
            pltpu.VMEM((512, 1024), BF16),
            pltpu.VMEM((2, 16, 8, 64, 128), BF16),
            pltpu.VMEM((256, 2048), F32),
            pltpu.VMEM((256, 16), F32),
            pltpu.VMEM((64, 2048), BF16),
            pltpu.VMEM((64, 2048), F32),
            dma((16,)),
            dma, dma((4,)),
            dma, dma((4,)),
            dma, dma((2 + PARTS,)),
            dma, dma((16,)),
            dma, dma((2,)),
            dma, dma((16,)),
            dma, dma((4,)),
            dma, dma((4, PARTS)),
            dma((4,)), dma((4,)),
            dma((3,)), dma((3,)),
            dma, dma,
        ],
        compiler_params=pltpu.CompilerParams(
            collective_id=0, has_side_effects=True, vmem_limit_bytes=60 * 1024 * 1024
        ),
        name="mixer_experts",
    )(
        pool_in, pool_weight, pool_gain.reshape(1, -1), out_weight, mix_gain.reshape(1, -1), expert_in, routes.T,
        route_weight.T, pre_gain.reshape(1, -1), gate_weight, up_weight, down_weight, post_gain.reshape(1, -1),
    )


def solution(mesh):
    return jax.shard_map(
        body,
        mesh=mesh,
        in_specs=(
            P(("ep", "tp"), None),
            P(),
            P(),
            P("tp", None),
            P(),
            P("ep", None),
            P("ep", None),
            P("ep", None),
            P(),
            P("ep", None, "tp"),
            P("ep", None, "tp"),
            P("ep", "tp", None),
            P(),
        ),
        out_specs=(P(("ep", "tp"), None), P(("ep", "tp"), None)),
        check_vma=False,
    )
```

```python
import functools

import jax
import jax.numpy as jnp
from jax import lax
from jax.experimental import pallas as pl
from jax.experimental.pallas import tpu as pltpu
from jax.sharding import PartitionSpec as P

MESH = pl.DeviceIdType.MESH
WINDOWS = (2, 4, 8, 16)
EPS = 1e-06
LIMIT = 7.0
ALPHA = 1.702
F32 = jnp.float32
BF16 = jnp.bfloat16


phase = jax.named_scope


FIRST = (1, 3, 2, 0)
SECOND = (2, 1, 3, 0)
OWN = 3
OTHERS = (0, 1, 2)
PARTS = 2


def clamped_unit(gate, up):
    gate = jnp.minimum(gate, LIMIT)
    up = jnp.clip(up, -LIMIT, LIMIT)
    return (up + 1.0) * gate * jax.nn.sigmoid(ALPHA * gate)


def remote(src, dst, send, recv, device):
    return pltpu.make_async_remote_copy(
        src_ref=src, dst_ref=dst, send_sem=send, recv_sem=recv, device_id=device, device_id_type=MESH
    )


def kernel(
    pool_in, pool_weight, pool_gain, out_weight, mix_gain, expert_in, routes, route_weight, pre_gain,
    gate_weight, up_weight, down_weight, post_gain,
    mix_out, expert_out,
    pool_w, pool_g, mix_g, pre_g, post_g, routes_v, route_w,
    tokens, picks, picks_in, sendbuf, rows_in, rows_z, part_in, part_z, sums, neigh, back, homebuf, homes,
    mine, theirs, gate_w, up_w, down_w, padded, mixed, w_all, acc, table, xin, own,
    local_sem, send_k, recv_k, send_m, recv_m, send_f, recv_f, send_a, recv_a, send_z, recv_z, send_p, recv_p, send_r, recv_r, send_t, recv_t,
    send_w, recv_w, send_o, recv_o, send_h, recv_h,
):
    i = lax.axis_index("ep")
    j = lax.axis_index("tp")
    z, c = j // 2, j % 2
    y, x = i // 4, i % 4
    p = z % 2
    here = (i, j)
    mate = (i, 2 * z + 1 - c)

    def plane(dy, dx):
        return ((y + dy) % 4) * 4 + (x + dx) % 4

    def turn(da, db):
        return plane(jnp.where(c == 0, da, db), jnp.where(c == 0, db, da))

    def along(dz):
        return (i, 2 * ((z + dz) % 8) + c)

    after = (jnp.where(j == 15, (i + 1) % 16, i), (j + 1) % 16)
    before = (jnp.where(j == 0, (i + 15) % 16, i), (j + 15) % 16)

    bar = pltpu.get_barrier_semaphore()

    def greet(device):
        pl.semaphore_signal(bar, inc=1, device_id=device, device_id_type=MESH)

    for d in range(1, 4):
        for core in range(2):
            greet((plane(d, 0), 2 * z + core))
            greet((plane(0, d), 2 * z + core))
    for dz in range(1, 8):
        greet(along(dz))
    greet(mate)
    greet((jnp.where(c == 1, after[0], before[0]), jnp.where(c == 1, after[1], before[1])))

    def block_row(parity, b):
        return pl.multiple_of((2 * (parity + 2 * b) + c) * 16, 16)

    loads = []

    def load(src, dst):
        copy = pltpu.make_async_copy(src, dst, local_sem.at[len(loads)])
        copy.start()
        loads.append(copy)
        return copy

    table_loads = [load(routes, routes_v), load(route_weight, route_w)]
    token_loads = [
        load(expert_in.at[pl.ds(block_row(1 - p, b), 16)], xin.at[pl.ds(16 * b, 16)]) for b in range(4)
    ]
    token_loads.append(load(pre_gain, pre_g))
    weight_loads = [
        load(gate_weight.at[c], gate_w.at[0]),
        load(up_weight.at[c], up_w.at[0]),
        load(down_weight.at[c], down_w.at[0]),
    ]
    gain_loads = [load(mix_gain, mix_g), load(post_gain, post_g)]
    pool_loads = [load(pool_weight, pool_w), load(pool_gain, pool_g)]
    pool_load = load(pool_in, padded.at[pl.ds(16, 512)])
    slow, fast = jnp.where(c == 0, y, x), jnp.where(c == 0, x, y)
    w_mine = slow * 4 + fast
    w_src = out_weight.at[:, pl.ds(pl.multiple_of(i * 128, 128), 128)]
    w_load = load(w_src, w_all.at[c, w_mine, z])

    lane = lax.broadcasted_iota(jnp.int32, (1, 512), 1)
    expert = jnp.zeros((1, 512), jnp.int32)
    for k in range(16):
        expert = jnp.where(lane // 32 == k, 2 * turn(FIRST[k // 4], SECOND[k % 4]), expert)
    expert = expert + (lane // 16) % 2
    slot_lane = lane % 16
    token = lax.broadcasted_iota(jnp.int32, (64, 64), 0)
    other = lax.broadcasted_iota(jnp.int32, (64, 64), 1)
    earlier = jnp.where((other < token) & (other // 16 == token // 16), 1.0, 0.0).astype(BF16)
    base = (lax.broadcasted_iota(jnp.int32, (64, 1), 0) // 16) * 4

    def turned(ref, column):
        block = jnp.concatenate([ref[...].astype(F32), jnp.zeros((4, 256), F32)], axis=0)
        table[:, column : column + 8] = block.T

    for copy in table_loads:
        copy.wait()
    turned(routes_v, 0)
    turned(route_w, 8)

    def selection(parity, weighted):
        rows = jnp.concatenate([table[pl.ds(block_row(parity, b), 16), :] for b in range(4)], axis=0)
        chosen, weights = rows[:, 0:4].astype(jnp.int32), rows[:, 8:12]
        hot = jnp.zeros((64, 512), F32)
        value = jnp.zeros((64, 512), F32)
        for k in range(4):
            match = chosen[:, k : k + 1] == expert
            hot = jnp.where(match, 1.0, hot)
            value = jnp.where(match, weights[:, k : k + 1], value)
        rank = jnp.dot(earlier, hot.astype(BF16), preferred_element_type=F32).astype(jnp.int32)
        taken = (rank + base) == slot_lane
        return jnp.where(taken, value if weighted else hot, 0.0)

    def landed(ref, sem):
        remote(ref, ref, send_h, sem, here).wait_recv()

    def left(ref, sem):
        remote(ref, ref, sem, recv_h, here).wait_send()

    def fill(a):
        pick = picks_in[a, 0:64].astype(F32).T.astype(BF16)
        rows = jnp.dot(pick, tokens[a], preferred_element_type=F32)
        sendbuf[4 * a : 4 * a + 4] = rows.astype(BF16).reshape(4, 2, 16, 2048)

    with phase("pack"):
        pick = selection(1 - p, False).astype(BF16)
        weight = selection(p, True)
        high = weight.astype(BF16)
        low = (weight - high.astype(F32)).astype(BF16)
        for a in range(4):
            lanes = slice(128 * a, 128 * a + 128)
            picks[a] = jnp.concatenate([pick[:, lanes], high[:, lanes], low[:, lanes]], axis=0)
        picks_in[OWN] = picks[OWN]
        for copy in token_loads:
            copy.wait()
        values = xin[...].astype(F32)
        scale = lax.rsqrt(jnp.mean(values * values, axis=-1, keepdims=True) + EPS)
        tokens[OWN] = (values * scale * pre_g[...]).astype(BF16)
        fill(OWN)

    with phase("barrier"):
        pl.semaphore_wait(bar, 21)

    def to_axis(a):
        device = (turn(FIRST[a], 0), j)
        return [
            remote(tokens.at[OWN], tokens.at[a], send_k, recv_k.at[a], device),
            remote(picks.at[a], picks_in.at[a], send_m, recv_m.at[a], device),
        ]

    def to_plane(k, core):
        return remote(
            sendbuf.at[k, core], rows_in.at[k, c], send_a, recv_a.at[k],
            (turn(0, SECOND[k % 4]), 2 * z + core),
        )

    def to_mate(k):
        return remote(sendbuf.at[k, 1 - c], rows_in.at[k, c], send_a, recv_a.at[k], mate)

    def pack(a):
        if a != OWN:
            for copy in to_axis(a):
                copy.wait_recv()
            fill(a)
        to_mate(4 * a + OWN).start()
        for b in OTHERS:
            for core in range(2):
                to_plane(4 * a + b, core).start()
        rows_in[4 * a + OWN, c] = sendbuf[4 * a + OWN, c]

    def axis():
        for a in OTHERS:
            for copy in to_axis(a):
                copy.start()

    def w_begin():
        for copy in w_z:
            copy.start()

    w_z = []
    for dz in range(1, 8):
        copy = remote(w_src, w_all.at[c, w_mine, z], send_w.at[0], recv_w.at[0], along(dz))
        w_z.append(copy)
    rim = remote(pool_in.at[pl.ds(496, 16)], padded.at[pl.ds(0, 16)], send_h, recv_h, after)
    swaps = [
        remote(gate_weight.at[1 - c], gate_w.at[1], send_o.at[0], recv_o.at[0], mate),
        remote(up_weight.at[1 - c], up_w.at[1], send_o.at[1], recv_o.at[1], mate),
        remote(down_weight.at[1 - c], down_w.at[1], send_o.at[2], recv_o.at[2], mate),
    ]

    def onward(k, core):
        return remote(
            rows_in.at[k, core], rows_z.at[k, core], send_z, recv_z.at[k // 8],
            along(1 if core == 0 else 7),
        )

    def arrive(ks):
        for k in ks:
            if k % 4 != OWN:
                landed(rows_in.at[k], recv_a.at[k])
            else:
                landed(rows_in.at[k, 1 - c], recv_a.at[k])
            for core in range(2):
                onward(k, core).start()

    def experts(source, first, count):
        block = source[first : first + count].reshape(32 * count, 2048)
        hidden = []
        for half in range(2):
            gate = jnp.dot(block, gate_w[half], preferred_element_type=F32)
            up = jnp.dot(block, up_w[half], preferred_element_type=F32)
            hidden.append(clamped_unit(gate, up).astype(BF16))
        hidden = jnp.concatenate(hidden, axis=1)
        return jnp.dot(hidden, down_w[...].reshape(512, 2048), preferred_element_type=F32)

    def partial(k, core):
        return remote(
            part_in.at[k, core], neigh.at[k, core], send_p, recv_p.at[k],
            along(1 if core == 0 else 7),
        )

    def inner(first, count):
        part = experts(rows_in, first, count)
        part_in[first : first + count] = part.astype(BF16).reshape(count, 2, 16, 2048)
        for k in range(first, first + count):
            for core in range(2):
                partial(k, core).start()

    def outer(first, count):
        landed(rows_z.at[pl.ds(first, count)], recv_z.at[first // 8])
        part_z[first : first + count] = experts(rows_z, first, count).reshape(count, 2, 16, 2048)

    def w_first():
        w_load.wait()
        landed(w_all.at[c, w_mine, pl.ds(0, 7)], recv_w.at[0])
        for k in range(1, 4):
            w_fast(k).start()

    def w_fast(k):
        dy, dx = jnp.where(c == 0, 0, k), jnp.where(c == 0, k, 0)
        return remote(w_all.at[c, w_mine], w_all.at[c, w_mine], send_w.at[1], recv_w.at[1], (plane(dy, dx), j))

    def w_slow(k):
        dy, dx = jnp.where(c == 0, k, 0), jnp.where(c == 0, 0, k)
        strip = w_all.at[c, pl.ds(slow * 4, 4)]
        return remote(strip, strip, send_w.at[2], recv_w.at[2], (plane(dy, dx), j))

    def w_core():
        return remote(w_all.at[c], w_all.at[c], send_w.at[3], recv_w.at[3], mate)

    def home(k, core):
        step_back = -SECOND[k % 4]
        there = plane(0, step_back) if core == 0 else plane(step_back, 0)
        return remote(
            sums.at[k, core], back.at[k, c], send_r, recv_r.at[k // 4], (there, 2 * z + core)
        )

    def home_mate(k):
        return remote(sums.at[k, 1 - c], back.at[k, c], send_r, recv_r.at[k // 4], mate)

    def settle(ks):
        for k in ks:
            landed(neigh.at[k], recv_p.at[k])
            sums[k] = (part_z[k] + neigh[k].astype(F32)).astype(BF16)
            if k % 4 != OWN:
                for core in range(2):
                    home(k, core).start()
            else:
                home_mate(k).start()
                back[k, c] = sums[k, c]

    def to_home(a):
        return remote(homebuf.at[a], homes.at[a], send_f, recv_f.at[a], (turn(-FIRST[a], 0), j))

    def cut(h):
        return pl.ds(h * (2048 // PARTS), 2048 // PARTS)

    def to_home_last(h):
        part = (2, slice(None), cut(h))
        return remote(homebuf.at[part], homes.at[part], send_f, recv_f.at[2 + h], (turn(-FIRST[2], 0), j))

    def combine(a):
        landed(back.at[pl.ds(0, 7), 0], recv_r.at[a])
        rows = back[4 * a : 4 * a + 4].reshape(128, 2048)
        both = jnp.dot(picks_in[a, 64:192], rows, preferred_element_type=F32)
        total = both[:64] + both[64:]
        if a != OWN:
            homebuf[a] = total.astype(BF16)
            for copy in [to_home_last(h) for h in range(PARTS)] if a == 2 else [to_home(a)]:
                copy.start()
        else:
            own[...] = total

    def mixer_first():
        for copy in pool_loads + [pool_load]:
            copy.wait()
        rim.wait_recv()
        number = i * 16 + j
        row = lax.broadcasted_iota(jnp.int32, (528, 1), 0)
        live = (row >= 16) | (number > 0)
        position = number * 512 + lax.broadcasted_iota(jnp.int32, (512, 1), 0)
        for g, window in enumerate(WINDOWS):
            inverse = 1.0 / jnp.minimum(position + 1, window).astype(F32)
            diffs = []
            for half in range(2):
                cols = slice(g * 256 + half * 128, g * 256 + half * 128 + 128)
                values = jnp.where(live, padded[:, cols].astype(F32), 0.0)
                total = values
                reach = 1
                while reach < window:
                    total = total + pltpu.roll(total, reach, 0)
                    reach *= 2
                diffs.append((total[16:] * inverse - values[16:]).astype(BF16))
            diff = jnp.concatenate(diffs, axis=1)
            out = jnp.dot(diff, pool_w[g], preferred_element_type=F32)
            mixed[:, g * 256 : (g + 1) * 256] = (out * pool_g[:, g * 256 : (g + 1) * 256]).astype(BF16)

    def w_strip():
        landed(w_all.at[c, pl.ds(0, 3)], recv_w.at[1])
        for k in range(1, 4):
            w_slow(k).start()

    def w_half():
        landed(w_all.at[c, pl.ds(0, 12)], recv_w.at[2])
        w_core().start()

    def weights():
        for copy in weight_loads:
            copy.wait()
        for copy in swaps:
            copy.wait_recv()

    def swap(n):
        swaps[n].start()

    def rim_begin():
        rim.start()

    def step(name, what, *args):
        with phase(name):
            what(*args)

    def mixer_second():
        for copy in gain_loads:
            copy.wait()
        w_core().wait_recv()
        for h in range(2):
            rows = mixed[256 * h : 256 * h + 256]
            square = jnp.zeros((256, 1), F32)
            for n in range(8):
                sides = []
                for b in (2 * n, 2 * n + 1):
                    turned = (b % 4) * 4 + b // 4
                    sides.append(
                        jnp.concatenate([w_all[core, (b, turned)[core], q] for q in range(8) for core in range(2)], axis=0)
                    )
                out = jnp.dot(rows, jnp.concatenate(sides, axis=1), preferred_element_type=F32)
                square = square + jnp.sum(out * out, axis=-1, keepdims=True)
                acc[:, 256 * n : 256 * n + 256] = out
            scale = lax.rsqrt(square * (1.0 / 2048.0) + EPS)
            mix_out[256 * h : 256 * h + 256] = (acc[...] * scale * mix_g[...]).astype(BF16)

    step("00_w_begin", w_begin)
    step("01_axis", axis)
    step("02_pack_3", pack, 3)
    step("03_rim_begin", rim_begin)
    step("04_arrive_15", arrive, (15,))
    step("05_swap_0", swap, 0)
    step("06_arrive_12_13_14", arrive, (12,13,14))
    step("07_pack_0", pack, 0)
    step("08_swap_1", swap, 1)
    step("09_pack_1", pack, 1)
    step("10_arrive_3_0_1_2", arrive, (3,0,1,2))
    step("11_swap_2", swap, 2)
    step("12_pack_2", pack, 2)
    step("13_w_first", w_first)
    step("14_arrive_7_4_5_6", arrive, (7,4,5,6))
    step("15_weights", weights)
    step("16_inner_0_8", inner, 0,8)
    step("17_arrive_11_8_9_10", arrive, (11,8,9,10))
    step("18_mixer_first", mixer_first)
    step("19_w_strip", w_strip)
    step("20_inner_8_8", inner, 8,8)
    step("21_outer_0_8", outer, 0,8)
    step("22_settle_0_1_2_3", settle, (0,1,2,3))
    step("23_settle_4_5_6_7", settle, (4,5,6,7))
    step("24_outer_8_8", outer, 8,8)
    step("25_combine_0", combine, 0)
    step("26_combine_1", combine, 1)
    step("27_w_half", w_half)
    step("28_settle_8_9_10_11", settle, (8,9,10,11))
    step("29_settle_12_13_14", settle, (12,13,14))
    step("30_combine_2", combine, 2)
    step("31_settle_15", settle, (15,))
    step("32_combine_3", combine, 3)
    def spread(m, h):
        return remote(
            mine.at[((z + 8 - 2 * m) % 8) // 2, :, cut(h)], theirs.at[m, :, cut(h)], send_t, recv_t.at[m, h],
            along(8 - 2 * m),
        )

    with phase("home"):
        total = own[...]
        for a in range(2):
            to_home(a).wait_recv()
            total = total + homes[a].astype(F32)
        own[...] = total
        for h in range(PARTS):
            to_home_last(h).wait_recv()
            part = own[:, cut(h)] + homes[2, :, cut(h)].astype(F32)
            mine[:, :, cut(h)] = part.astype(BF16).reshape(4, 16, 2048 // PARTS)
            for m in (2, 1, 3):
                spread(m, h).start()
            own[:, cut(h)] = part

    with phase("reduce"):
        mixer_second()
        result = own[pl.ds(pl.multiple_of((z // 2) * 16, 16), 16), :]
        for m in (1, 3, 2):
            for h in range(PARTS):
                spread(m, h).wait_recv()
            result = result + theirs[m].astype(F32)

    with phase("norm"):
        scale = lax.rsqrt(jnp.mean(result * result, axis=-1, keepdims=True) + EPS)
        expert_out[...] = (result * scale * post_g[...]).astype(BF16)

    with phase("drain"):
        for copy in swaps + [rim, w_core()]:
            copy.wait_send()
        left(tokens.at[pl.ds(0, 3)], send_k)
        left(picks.at[pl.ds(0, 3)], send_m)
        left(homebuf.at[pl.ds(0, 3)], send_f)
        left(mine.at[pl.ds(0, 3)], send_t)
        left(w_all.at[c, w_mine, pl.ds(0, 7)], send_w.at[0])
        left(w_all.at[c, pl.ds(0, 3)], send_w.at[1])
        left(w_all.at[c, pl.ds(0, 12)], send_w.at[2])
        left(sendbuf.at[pl.ds(0, 14)], send_a)
        left(rows_in, send_z)
        left(part_in, send_p)
        left(sums.at[pl.ds(0, 14)], send_r)


def write_out(mix, expert, mix_out, expert_out, sem):
    copies = [pltpu.make_async_copy(expert, expert_out, sem.at[4])]
    for n in range(4):
        part = pl.ds(128 * n, 128)
        copies.append(pltpu.make_async_copy(mix.at[part], mix_out.at[part], sem.at[n]))
    for copy in copies:
        copy.start()
    for copy in copies:
        copy.wait()


def body(
    pool_in, pool_weight, pool_gain, out_weight, mix_gain, expert_in, routes, route_weight, pre_gain,
    gate_weight, up_weight, down_weight, post_gain,
):
    vmem = pl.BlockSpec(memory_space=pltpu.VMEM)
    hbm = pl.BlockSpec(memory_space=pl.ANY)
    dma = pltpu.SemaphoreType.DMA
    tile = (16, 2, 16, 2048)
    mix, expert = pl.pallas_call(
        kernel,
        out_shape=(
            pltpu.VMEM((512, 2048), BF16),
            pltpu.VMEM((16, 2048), BF16),
        ),
        in_specs=[hbm] * 13,
        out_specs=(vmem, vmem),
        scratch_shapes=[
            pltpu.VMEM((4, 256, 256), BF16),
            pltpu.VMEM((1, 1024), F32),
            pltpu.VMEM((1, 2048), F32),
            pltpu.VMEM((1, 2048), F32),
            pltpu.VMEM((1, 2048), F32),
            pltpu.VMEM((4, 256), jnp.int32),
            pltpu.VMEM((4, 256), F32),
            pltpu.VMEM((4, 64, 2048), BF16),
            pltpu.VMEM((4, 192, 128), BF16),
            pltpu.VMEM((4, 192, 128), BF16),
            pltpu.VMEM(tile, BF16),
            pltpu.VMEM(tile, BF16),
            pltpu.VMEM(tile, BF16),
            pltpu.VMEM(tile, BF16),
            pltpu.VMEM(tile, F32),
            pltpu.VMEM(tile, BF16),
            pltpu.VMEM(tile, BF16),
            pltpu.VMEM(tile, BF16),
            pltpu.VMEM((4, 64, 2048), BF16),
            pltpu.VMEM((4, 64, 2048), BF16),
            pltpu.VMEM((4, 16, 2048), BF16),
            pltpu.VMEM((4, 16, 2048), BF16),
            pltpu.VMEM((2, 2048, 256), BF16),
            pltpu.VMEM((2, 2048, 256), BF16),
            pltpu.VMEM((2, 256, 2048), BF16),
            pltpu.VMEM((528, 1024), BF16),
            pltpu.VMEM((512, 1024), BF16),
            pltpu.VMEM((2, 16, 8, 64, 128), BF16),
            pltpu.VMEM((256, 2048), F32),
            pltpu.VMEM((256, 16), F32),
            pltpu.VMEM((64, 2048), BF16),
            pltpu.VMEM((64, 2048), F32),
            dma((16,)),
            dma, dma((4,)),
            dma, dma((4,)),
            dma, dma((2 + PARTS,)),
            dma, dma((16,)),
            dma, dma((2,)),
            dma, dma((16,)),
            dma, dma((4,)),
            dma, dma((4, PARTS)),
            dma((4,)), dma((4,)),
            dma((3,)), dma((3,)),
            dma, dma,
        ],
        compiler_params=pltpu.CompilerParams(
            collective_id=0, has_side_effects=True, vmem_limit_bytes=60 * 1024 * 1024
        ),
        name="mixer_experts",
    )(
        pool_in, pool_weight, pool_gain.reshape(1, -1), out_weight, mix_gain.reshape(1, -1), expert_in, routes.T,
        route_weight.T, pre_gain.reshape(1, -1), gate_weight, up_weight, down_weight, post_gain.reshape(1, -1),
    )
    return pl.pallas_call(
        write_out,
        out_shape=(
            jax.ShapeDtypeStruct((512, 2048), BF16),
            jax.ShapeDtypeStruct((16, 2048), BF16),
        ),
        in_specs=[hbm, hbm],
        out_specs=(hbm, hbm),
        scratch_shapes=[dma((5,))],
        compiler_params=pltpu.CompilerParams(vmem_limit_bytes=1024 * 1024),
        name="write_out",
    )(mix, expert)


def solution(mesh):
    return jax.shard_map(
        body,
        mesh=mesh,
        in_specs=(
            P(("ep", "tp"), None),
            P(),
            P(),
            P("tp", None),
            P(),
            P("ep", None),
            P("ep", None),
            P("ep", None),
            P(),
            P("ep", None, "tp"),
            P("ep", None, "tp"),
            P("ep", "tp", None),
            P(),
        ),
        out_specs=(P(("ep", "tp"), None), P(("ep", "tp"), None)),
        check_vma=False,
    )
```
